32 devices in a mesh: fs: 16 (over z, y, core), tp: 2 (over x).
Axes of the slice: x: 2, y: 2, z: 4, core: 2. Of those that a mesh axis runs over, the one named last changes fastest.
Arguments:
- saved_input: bfloat16 [8192, 3072], P('fs'), may hold values from -6 to 6
- output_cotangent: bfloat16 [8192, 3072], P('fs'), may hold values from -6 to 6
- recurrent_output: bfloat16 [8192, 1536], P('fs', 'tp'), may hold values from -6 to 6
- forget_logit: bfloat16 [8192, 1536], P('fs', 'tp'), may hold values from -12 to 12
- forget_cotangent: bfloat16 [8192, 1536], P('fs', 'tp'), may hold values from -6 to 6
- lower_bound: float32 [1536], P('tp'), may hold values from 0.2 to 0.9
- basis_in: bfloat16 [3072, 384], P('fs'), may hold values from -1.2629537 to 1.2629537
- basis_out: bfloat16 [3072, 384], P('fs'), may hold values from -1.2629537 to 1.2629537
- moment_in: float32 [384, 1536], P('fs', 'tp'), may hold values from -6 to 6
- second_in: float32 [384, 1536], P('fs', 'tp'), may hold values from 0.25 to 4
- moment_out: float32 [384, 1536], P('fs', 'tp'), may hold values from -6 to 6
- second_out: float32 [384, 1536], P('fs', 'tp'), may hold values from 0.25 to 4
- weight_in: float32 [3072, 1536], P('fs', 'tp'), may hold values from -0.109375 to 0.109375
- weight_out: float32 [1536, 3072], P('tp', 'fs'), may hold values from -0.15625 to 0.15625
Outputs:
- moment_in_new: float32 [384, 1536], P('fs', 'tp')
- second_in_new: float32 [384, 1536], P('fs', 'tp')
- moment_out_new: float32 [384, 1536], P('fs', 'tp')
- second_out_new: float32 [384, 1536], P('fs', 'tp')
- weight_in_new: float32 [3072, 1536], P('fs', 'tp')
- weight_out_new: float32 [1536, 3072], P('tp', 'fs')
- copy_in: bfloat16 [3072, 1536], P(None, 'tp')
- copy_out: bfloat16 [1536, 3072], P('tp')
The draws below stay inside these ranges and needn't reach their ends.
All inputs are finite; a program needn't handle non-finite values.
Results may differ from the reference program's by a relative error of at most 0.0023.
Values may be sent and summed in bfloat16 or wider, within the bound.
A program may use at most 64 MiB of HBM per device.

```python
import math
import jax
import jax.numpy as jnp
from jax import lax

D = 3072
HW = 1536
R = 384
TOKENS = 8192


def scaled_basis(key):
    first, second = jax.random.split(key)
    ramp = 10.0 ** (jnp.arange(R, dtype=jnp.float32) / R)
    jitter = jax.random.uniform(first, (R,), jnp.float32, 0.7, 1.4)
    values = jnp.clip(jax.random.normal(second, (D, R), jnp.float32), -5.0, 5.0)
    return (values * ramp[None, :] * jitter[None, :] * D ** (-0.5)).astype(jnp.bfloat16)


def draw_basis_in(key, part):
    return scaled_basis(jax.random.fold_in(key, 11))


def draw_basis_out(key, part):
    return scaled_basis(jax.random.fold_in(key, 23))


def levels(rng, shape, cuts, smallest, top_value):
    level = 1.0
    for position, blocks in cuts:
        steps = jax.random.uniform(jax.random.fold_in(jax.random.fold_in(rng, 6), position), (blocks,), jnp.float32, smallest / len(cuts), top_value / len(cuts))
        level = level * jnp.repeat(jnp.exp(steps), shape[position] // blocks).reshape((-1,) + (1,) * (len(shape) - 1 - position))
    return level


def centred(key, extent, scale, most, cuts=(), held_as=jnp.bfloat16):
    values = jax.random.normal(key, extent, jnp.float32) * scale
    if len(cuts) > 0:
        values = levels(key, extent, cuts, -0.22, 0.18) * values
    return jnp.clip(values, min=-most, max=most).astype(held_as)


def setup_inputs(seed: int = 0) -> dict:
    key_of = jax.random.split(jax.random.key(seed), 15)
    saved_input = centred(key_of[0], (TOKENS, D), 1.0, 6.0, ((0, 16),))
    output_cotangent = centred(key_of[1], (TOKENS, D), 1.0, 6.0, ((0, 16),))
    recurrent_output = centred(key_of[2], (TOKENS, HW), 1.0, 6.0, ((0, 16), (1, 2)))
    forget_logit = centred(key_of[3], (TOKENS, HW), 2.0, 12.0, ((0, 16), (1, 2)))
    forget_cotangent = centred(key_of[4], (TOKENS, HW), 1.0, 6.0, ((0, 16), (1, 2)))
    lower_bound = jnp.clip(0.2 + 0.7 * jax.random.uniform(key_of[5], (HW,), jnp.float32) ** levels(key_of[5], (HW,), ((0, 2),), -0.2, 0.2), 0.2, 0.9)
    basis_in = draw_basis_in(jax.random.fold_in(key_of[14], 71), 0)
    basis_out = draw_basis_out(jax.random.fold_in(key_of[14], 71), 0)
    moment_in = centred(key_of[8], (R, HW), 1.0, 6.0, ((0, 16), (1, 2)), jnp.float32)
    second_in = jnp.clip(jnp.exp(math.log(4.0) - 2.7725887 * jax.random.uniform(key_of[9], (R, HW), jnp.float32) ** levels(key_of[9], (R, HW), ((0, 16), (1, 2)), -0.2, 0.2)), 0.25, 4.0)
    moment_out = centred(key_of[10], (R, HW), 1.0, 6.0, ((0, 16), (1, 2)), jnp.float32)
    second_out = jnp.clip(jnp.exp(math.log(4.0) - 2.7725887 * jax.random.uniform(key_of[11], (R, HW), jnp.float32) ** levels(key_of[11], (R, HW), ((0, 16), (1, 2)), -0.2, 0.2)), 0.25, 4.0)
    weight_in = centred(key_of[12], (D, HW), D ** -0.5, 0.109375, ((0, 16), (1, 2)), jnp.float32)
    weight_out = centred(key_of[13], (HW, D), HW ** -0.5, 0.15625, ((0, 2), (1, 16)), jnp.float32)
    return {"saved_input": saved_input, "output_cotangent": output_cotangent, "recurrent_output": recurrent_output, "forget_logit": forget_logit, "forget_cotangent": forget_cotangent, "lower_bound": lower_bound, "basis_in": basis_in, "basis_out": basis_out, "moment_in": moment_in, "second_in": second_in, "moment_out": moment_out, "second_out": second_out, "weight_in": weight_in, "weight_out": weight_out}


def reference(saved_input, output_cotangent, recurrent_output, forget_logit, forget_cotangent, lower_bound, basis_in, basis_out, moment_in, second_in, moment_out, second_out, weight_in, weight_out):
    sig = jax.nn.sigmoid(forget_logit.astype(jnp.float32))
    gate_cot = (forget_cotangent.astype(jnp.float32) * (1.0 - lower_bound)[None, :] * sig * (1.0 - sig)).astype(jnp.bfloat16)
    coded_in = jnp.dot(saved_input, basis_in, preferred_element_type=jnp.float32).astype(jnp.bfloat16)
    coded_out = jnp.dot(output_cotangent, basis_out, preferred_element_type=jnp.float32).astype(jnp.bfloat16)
    low_in = jnp.dot(coded_in.T, gate_cot, preferred_element_type=jnp.float32)
    low_out = jnp.dot(coded_out.T, recurrent_output, preferred_element_type=jnp.float32)
    total = jnp.sum(low_in * low_in) + jnp.sum(low_out * low_out)
    clip = jnp.minimum(1.0, jnp.sqrt(jnp.float32(2 * R * HW)) * lax.rsqrt(total + 1e-06))
    grad_in = clip * low_in
    grad_out = clip * low_out
    moment_in_new = 0.8 * moment_in + 0.2 * grad_in
    moment_out_new = 0.8 * moment_out + 0.2 * grad_out
    second_in_new = 0.9 * second_in + 0.1 * grad_in * grad_in
    second_out_new = 0.9 * second_out + 0.1 * grad_out * grad_out
    step_in = moment_in_new / (jnp.sqrt(second_in_new) + 1e-08)
    step_out = moment_out_new / (jnp.sqrt(second_out_new) + 1e-08)
    update_in = jnp.dot(basis_in.astype(jnp.float32), step_in, precision=lax.Precision.HIGHEST)
    update_out = jnp.dot(step_out.T, basis_out.astype(jnp.float32).T, precision=lax.Precision.HIGHEST)
    weight_in_new = weight_in - 0.01 * update_in
    weight_out_new = weight_out - 0.01 * update_out
    return (moment_in_new, second_in_new, moment_out_new, second_out_new, weight_in_new, weight_out_new, weight_in_new.astype(jnp.bfloat16), weight_out_new.astype(jnp.bfloat16))
```

```python
import functools

import jax
import jax.numpy as jnp
from jax import lax
from jax.experimental import pallas as pl
from jax.experimental.pallas import tpu as pltpu
from jax.sharding import PartitionSpec as P

MESH = pl.DeviceIdType.MESH
F32 = jnp.float32
BF16 = jnp.bfloat16
UNROLL = 16
TILE = 128


def loop(start, stop, body):
    if stop - start <= UNROLL:
        for i in range(start, stop):
            body(i)
    else:

        @pl.loop(start, stop)
        def _(i):
            body(i)


def mod(value, n):
    return lax.rem(value + 2 * n, n)


def kernel(
    nf,
    nt,
    limit,
    x_hbm,
    y_hbm,
    rec_hbm,
    logit_hbm,
    fcot_hbm,
    lower_ref,
    basis_in_hbm,
    basis_out_hbm,
    m_in,
    s_in,
    m_out,
    s_out,
    w_in,
    w_out,
    mn_in,
    sn_in,
    mn_out,
    sn_out,
    wn_in,
    wn_out,
    copy_in,
    copy_out,
    data,
    logit,
    fcot,
    cots,
    bas,
    own_bas,
    coded,
    term,
    part,
    peer,
    hop,
    step,
    flat,
    small,
    fresh,
    old,
    new,
    cp,
    tots,
    load_sem,
    base_sem,
    out_sem,
    send_a,
    ring_a,
    pair_a,
    send_b,
    ring_b,
    sum_sem,
    swap_sem,
    tot_sem,
    send_d,
    ring_d,
    pair_d,
    send_f,
    ring_f,
    pair_f,
):
    f = lax.axis_index("fs")
    tp = lax.axis_index("tp")
    q = lax.rem(tp, 2)
    n = nf // 2
    z = n // 2
    core = lax.rem(f, 2)
    chip = f // 2
    row, column = chip // 2, lax.rem(chip, 2)
    me = (1 - column) * row + column * (n - 1 - row)
    partner = (f + 1 - 2 * core, tp)
    across = (f, tp + 1 - 2 * q)

    def chip_at(position):
        side = position // z
        return 2 * ((1 - side) * position + side * (n - 1 - position)) + side

    def dev_at(position):
        return chip_at(position) * 2 + core

    depth = basis_in_hbm.shape[0]
    half = depth // 2
    units = cots.shape[2]
    span = part.shape[2]
    lanes = 2 if units % 256 == 0 else 1
    width = units // lanes

    def own(ref, dev):
        return ref.at[pl.ds(pl.multiple_of(dev * depth, depth), depth)]

    def fetch(src, dst, i):
        return pltpu.make_async_copy(src, dst, load_sem.at[i])

    def pick(i, first, second, dst, sem):
        @pl.when(q == 0)
        def _():
            pltpu.make_async_copy(first, dst, sem).start()

        @pl.when(q == 1)
        def _():
            pltpu.make_async_copy(second, dst, sem).start()

        return pltpu.make_async_copy(first, dst, sem)

    own_load = pick(0, basis_in_hbm, basis_out_hbm, own(bas, f), base_sem.at[0])
    gate_loads = [fetch(logit_hbm, logit, 0), fetch(fcot_hbm, fcot, 1)]
    for copy in gate_loads:
        copy.start()
    data_load = pick(1, x_hbm, y_hbm, data, base_sem.at[1])
    late_loads = [
        fetch(src, dst, 2 + i)
        for i, (src, dst) in enumerate(
            (
                (rec_hbm, cots.at[1]),
                (m_in, small.at[0]),
                (s_in, small.at[1]),
                (m_out, small.at[2]),
                (s_out, small.at[3]),
                (basis_in_hbm, own_bas.at[0]),
                (basis_out_hbm, own_bas.at[1]),
                (w_in, old.at[0]),
                (w_out, old.at[1]),
            )
        )
    ]
    for copy in late_loads:
        copy.start()

    barrier = pltpu.get_barrier_semaphore()
    everyone = nf * nt
    my_id = f * nt + tp

    def other(i):
        target = lax.rem(my_id + i, everyone)
        return (target // nt, lax.rem(target, nt))

    @pl.loop(1, everyone)
    def _(i):
        pl.semaphore_signal(barrier, inc=1, device_id=other(i), device_id_type=MESH)

    pl.semaphore_wait(barrier, everyone - 1)

    far = n // 2
    near = n - 1 - far
    two_way = ((0, 1, far), (1, -1, far), (0, -1, near), (1, 1, near))

    def neighbour(way):
        return (dev_at(mod(me + way, n)), tp)

    def send(src, dst, sems, target):
        return pltpu.make_async_remote_copy(
            src_ref=src,
            dst_ref=dst,
            send_sem=sems[0],
            recv_sem=sems[1],
            device_id=target,
            device_id_type=MESH,
        )

    def gather(view, chunks, send_sem, ring_sem, pair_sem, between=None):
        flows = two_way

        def remote(j, s, c, sems, target):
            t, way, _ = flows[j]
            block = view(t, dev_at(mod(me - way * s, n)), c)
            return send(block, block, sems, target)

        def ring_copy(j, s, c):
            sems = send_sem.at[j, s, c], ring_sem.at[j, s, c]
            return remote(j, s, c, sems, neighbour(flows[j][1]))

        def pair_copy(j, s, c):
            sems = pair_sem.at[0, j, s, c], pair_sem.at[1, j, s, c]
            return remote(j, s, c, sems, partner)

        def each(s, act):
            for c in range(chunks):
                for j in range(len(flows)):
                    act(j, s, c)

        def move(j, s, c, first=False, last=False):
            if not first:
                ring_copy(j, s - 1, c).wait_recv()
            if not last:
                ring_copy(j, s, c).start()
            if not first or j < 2:
                pair_copy(j, s, c).start()

        each(0, functools.partial(move, first=True))
        if between is not None:
            between()
        loop(1, near, lambda s: each(s, move))
        for s in range(near, far + 1):
            for c in range(chunks):
                for j, (_, _, hops) in enumerate(flows):
                    if s <= hops:
                        move(j, s, c, last=s == hops)

        def finish(j, s, c):
            pair_copy(j, s, c).wait()

        def sent(j, s, c):
            ring_copy(j, s, c).wait_send()

        for c in range(chunks):
            for j, (_, _, hops) in enumerate(flows):
                if j < 2:
                    finish(j, 0, c)
                for s in range(near, hops):
                    sent(j, s, c)
                for s in range(near, hops + 1):
                    finish(j, s, c)
        loop(1, near, lambda s: each(s, finish))
        loop(0, near, lambda s: each(s, sent))

    def make_gate():
        for copy in gate_loads:
            copy.wait()
        tile = 64

        @pl.loop(0, cots.shape[1] // tile)
        def _(i):
            at = pl.ds(pl.multiple_of(i * tile, tile), tile)
            for k in range(units // TILE):
                to = slice(k * TILE, (k + 1) * TILE)
                sig = jax.nn.sigmoid(logit[at, to].astype(F32))
                cots[0, at, to] = (
                    fcot[at, to].astype(F32)
                    * (1.0 - lower_ref[k : k + 1, :])
                    * sig
                    * (1.0 - sig)
                ).astype(BF16)

    own_load.wait()
    gather(
        lambda t, dev, c: bas.at[
            pl.ds(pl.multiple_of(dev * depth + t * half, half), half)
        ],
        1,
        send_a,
        ring_a,
        pair_a,
        make_gate,
    )
    data_load.wait()

    def piece(i):
        return pl.ds(pl.multiple_of(i * TILE, TILE), TILE)

    def swap(i):
        sems = swap_sem.at[0, i], swap_sem.at[1, i]
        return send(coded.at[0, piece(i)], coded.at[1, piece(i)], sems, across)

    tiles = data.shape[0] // TILE

    @pl.loop(0, tiles)
    def _(i):
        coded[0, piece(i)] = jnp.dot(
            data[piece(i)], bas[...], preferred_element_type=F32
        ).astype(BF16)
        swap(i).start()

    def project(k):
        t = q if k == 0 else 1 - q
        for c in range(lanes):
            at = slice(c * width, (c + 1) * width)
            term[:, at] = lax.dot_general(
                coded[k], cots[t, :, at], (((0,), (0,)), ((), ())), preferred_element_type=F32
            )
        for i in range(nf):
            part[k * 2 + i % 2, i // 2] = term[i * span : (i + 1) * span]

    def pair_sum(k):
        sems = sum_sem.at[0, k], sum_sem.at[1, k]
        return send(part.at[k * 2 + 1 - core], peer.at[k], sems, partner)

    def ring_add(j, s, c):
        at = pl.ds(c * width, width)
        sems = send_b.at[j, s, c], ring_b.at[j, s, c]
        return send(hop.at[j, s, :, at], hop.at[j, s + 1, :, at], sems, neighbour(two_way[j][1]))

    def mine(j, s, c):
        k, way, hops = two_way[j]
        at = pl.ds(c * width, width)
        place = chip_at(mod(me + way * (hops - s), n))
        return part[k * 2 + core, place, :, at] + peer[k, place, :, at]

    def begin(k):
        pair_sum(k).wait_recv()
        for c in range(lanes):
            at = pl.ds(c * width, width)
            for j in (k, k + 2):
                if two_way[j][2] > 0:
                    hop[j, 0, :, at] = mine(j, 0, c)
                    ring_add(j, 0, c).start()

    def relay(j, s, c):
        at = pl.ds(c * width, width)
        ring_add(j, s - 1, c).wait_recv()
        hop[j, s, :, at] = hop[j, s, :, at] + mine(j, s, c)
        ring_add(j, s, c).start()

    def relay_all(k, s):
        for c in range(lanes):
            for j in (k, k + 2):
                if isinstance(s, int) and s >= two_way[j][2]:
                    continue
                relay(j, s, c)

    def settle_sum(k):
        for c in range(lanes):
            at = pl.ds(c * width, width)
            ring_add(k + 2, near - 1, c).wait_recv()
            kept = hop[k + 2, near, :, at] + mine(k + 2, near, c)
            ring_add(k, far - 1, c).wait_recv()
            hop[k, far, :, at] = hop[k, far, :, at] + kept

    late_loads[0].wait()
    project(0)
    pair_sum(0).start()
    begin(0)
    early = max(1, near - 1)
    loop(1, early, lambda s: relay_all(0, s))

    @pl.loop(0, tiles)
    def _(i):
        swap(i).wait_recv()

    project(1)
    pair_sum(1).start()
    for s in range(early, far):
        relay_all(0, s)
    begin(1)
    settle_sum(0)
    loop(1, near, lambda s: relay_all(1, s))
    for s in range(near, far):
        relay_all(1, s)
    settle_sum(1)

    low = [hop[k, far] for k in range(2)]
    square = jnp.sum(low[0] * low[0] + low[1] * low[1], axis=(0, 1), keepdims=True)
    tots[my_id] = jnp.broadcast_to(square, tots.shape[1:])

    def tell(i):
        return send(tots.at[my_id], tots.at[my_id], (tot_sem.at[0], tot_sem.at[1]), other(i))

    @pl.loop(1, everyone)
    def _(i):
        tell(i).start()

    def sent_all(s):
        for c in range(lanes):
            for j in range(4):
                ring_add(j, s, c).wait_send()

    loop(0, near, sent_all)
    for s in range(near, far):
        for c in range(lanes):
            for j in range(2):
                ring_add(j, s, c).wait_send()
    for k in range(2):
        pair_sum(k).wait_send()

    @pl.loop(0, tiles)
    def _(i):
        swap(i).wait_send()

    for copy in late_loads[1:]:
        copy.wait()
    all_tots = tots.at[pl.ds(0, everyone - 1)]
    pltpu.make_async_copy(all_tots, all_tots, tot_sem.at[1]).wait()
    pltpu.make_async_copy(all_tots, all_tots, tot_sem.at[0]).wait()

    total = jnp.sum(tots[...], axis=0)
    clip = jnp.minimum(1.0, jnp.sqrt(F32(limit)) * lax.rsqrt(total + 1e-06))[0:1, 0:1]
    for t in range(2):
        grad = clip * hop[lax.rem(q + t, 2), far]
        moment = 0.8 * small[2 * t] + 0.2 * grad
        second = 0.9 * small[2 * t + 1] + 0.1 * grad * grad
        fresh[2 * t] = moment
        fresh[2 * t + 1] = second
        step[t, f] = moment / (jnp.sqrt(second) + 1e-08)

    puts = [
        pltpu.make_async_copy(fresh.at[i], dst, out_sem.at[i])
        for i, dst in enumerate((mn_in, sn_in, mn_out, sn_out))
    ] + [
        pltpu.make_async_copy(new.at[t], dst, out_sem.at[4 + t])
        for t, dst in enumerate((wn_in, wn_out))
    ]

    gather(
        lambda t, dev, c: step.at[t, dev, :, pl.ds(c * width, width)],
        lanes,
        send_d,
        ring_d,
        pair_d,
    )
    for copy in puts[:4]:
        copy.start()

    cut = send_f.shape[2]
    slab = depth // cut
    ways = (1, -1)

    def block(t, s, c):
        dev = dev_at(mod(me - ways[t] * s, n))
        return cp.at[t, pl.ds(pl.multiple_of(dev * depth + c * slab, slab), slab)]

    def pass_on(t, s, c):
        sems = send_f.at[t, s, c], ring_f.at[t, s, c]
        return send(block(t, s, c), block(t, s, c), sems, neighbour(ways[t]))

    def share(t, s, c):
        sems = pair_f.at[0, t, s, c], pair_f.at[1, t, s, c]
        return send(block(t, s, c), block(t, s, c), sems, partner)

    outs = (copy_in, copy_out)

    def put(t, s):
        place = chip_at(mod(me - ways[t] * s, n))
        rows = pl.ds(pl.multiple_of(place * 2 * depth, 2 * depth), 2 * depth)
        return pltpu.make_async_copy(
            cp.at[t, rows], outs[t].at[rows], out_sem.at[6 + t]
        )

    for t in range(2):
        for k in range(nf):
            flat[k * span : (k + 1) * span] = step[t, k]
        whole = flat[...]
        high = whole.astype(BF16)
        rest = (whole - high.astype(F32)).astype(BF16)
        mat = own_bas[t]
        update = jnp.dot(mat, rest, preferred_element_type=F32) + jnp.dot(
            mat, high, preferred_element_type=F32
        )
        made = old[t] - 0.01 * update
        new[t] = made
        cp[t, pl.ds(pl.multiple_of(f * depth, depth), depth)] = made.astype(BF16)
        for c in range(cut):
            pass_on(t, 0, c).start()
        for c in range(cut):
            share(t, 0, c).start()
    for copy in puts[4:]:
        copy.start()

    def gone(s):
        for t in range(2):
            for c in range(cut):
                share(t, s, c).wait()
            put(t, s).start()

    def forward(s):
        for c in range(cut):
            for t in range(2):
                pass_on(t, s - 1, c).wait_recv()
                pass_on(t, s, c).start()
                share(t, s, c).start()
        gone(s - 1)

    loop(1, n - 1, forward)
    for c in range(cut):
        for t in range(2):
            pass_on(t, n - 2, c).wait_recv()
            share(t, n - 1, c).start()
    gone(n - 2)
    gone(n - 1)

    def left(s):
        for c in range(cut):
            for t in range(2):
                pass_on(t, s, c).wait_send()

    loop(0, n - 1, left)
    for copy in puts:
        copy.wait()
    for t in range(2):
        pltpu.make_async_copy(cp.at[t], outs[t], out_sem.at[6 + t]).wait()


def settle(*refs):
    ins, outs = refs[:8], refs[8:16]
    held, tall, wide, in_sem, out_sem = refs[16:22], refs[22], refs[23], refs[24], refs[25]
    blocks = tall.shape[1]
    size = tall.shape[2]

    def rows(i):
        return pl.ds(i * size, size)

    def get(t, i):
        return pltpu.make_async_copy(ins[6 + t].at[rows(i)], tall.at[t, i], in_sem.at[t, i])

    def put(t, i):
        if t == 0:
            return pltpu.make_async_copy(tall.at[0, i], outs[6].at[rows(i)], out_sem.at[0, i])
        return pltpu.make_async_copy(
            wide.at[:, rows(i)], outs[7].at[:, rows(i)], out_sem.at[1, i]
        )

    more = [
        (
            pltpu.make_async_copy(src, mid, in_sem.at[2, i]),
            pltpu.make_async_copy(mid, dst, out_sem.at[2, i]),
        )
        for i, (src, mid, dst) in enumerate(zip(ins[:6], held, outs[:6]))
    ]
    for i in range(blocks):
        for t in (1, 0):
            get(t, i).start()
    for load, _ in more:
        load.start()
    for i in range(blocks):
        get(1, i).wait()
        wide[:, rows(i)] = tall[1, i].T
        put(1, i).start()
        get(0, i).wait()
        put(0, i).start()
    for load, save in more:
        load.wait()
        save.start()
    for i in range(blocks):
        for t in (1, 0):
            put(t, i).wait()
    for _, save in more:
        save.wait()


def body(
    saved_input,
    output_cotangent,
    recurrent_output,
    forget_logit,
    forget_cotangent,
    lower_bound,
    basis_in,
    basis_out,
    moment_in,
    second_in,
    moment_out,
    second_out,
    weight_in,
    weight_out,
):
    nf, nt = lax.axis_size("fs"), lax.axis_size("tp")
    n = nf // 2
    tokens, model = saved_input.shape
    units = recurrent_output.shape[1]
    depth, rank = basis_in.shape
    span = moment_in.shape[0]
    limit = 2.0 * rank * units * nt
    small = jax.ShapeDtypeStruct((span, units), F32)
    weight = jax.ShapeDtypeStruct((depth, units), F32)
    copied = jax.ShapeDtypeStruct((model, units), BF16)
    cut = 2 if depth % 32 == 0 else 1
    lanes = 2 if units % 256 == 0 else 1
    far = n // 2
    hbm = pl.BlockSpec(memory_space=pl.ANY)
    vmem = pl.BlockSpec(memory_space=pltpu.VMEM)
    dma = pltpu.SemaphoreType.DMA
    outs = pl.pallas_call(
        functools.partial(kernel, nf, nt, limit),
        out_shape=(small, small, small, small, weight, weight, copied, copied),
        in_specs=[hbm] * 5 + [vmem] + [hbm] * 8,
        out_specs=[hbm] * 8,
        scratch_shapes=[
            pltpu.VMEM((tokens, model), BF16),
            pltpu.VMEM((tokens, units), BF16),
            pltpu.VMEM((tokens, units), BF16),
            pltpu.VMEM((2, tokens, units), BF16),
            pltpu.VMEM((model, rank), BF16),
            pltpu.VMEM((2, depth, rank), BF16),
            pltpu.VMEM((2, tokens, rank), BF16),
            pltpu.VMEM((rank, units), F32),
            pltpu.VMEM((4, n, span, units), F32),
            pltpu.VMEM((2, n, span, units), F32),
            pltpu.VMEM((4, far + 1, span, units), F32),
            pltpu.VMEM((2, nf, span, units), F32),
            pltpu.VMEM((rank, units), F32),
            pltpu.VMEM((4, span, units), F32),
            pltpu.VMEM((4, span, units), F32),
            pltpu.VMEM((2, depth, units), F32),
            pltpu.VMEM((2, depth, units), F32),
            pltpu.VMEM((2, model, units), BF16),
            pltpu.VMEM((nf * nt, 8, 128), F32),
            dma((11,)),
            dma((2,)),
            dma((8,)),
            dma((4, far, 1)),
            dma((4, far, 1)),
            dma((2, 4, far + 1, 1)),
            dma((4, far, lanes)),
            dma((4, far, lanes)),
            dma((2, 2)),
            dma((2, tokens // TILE)),
            dma((2,)),
            dma((4, far, lanes)),
            dma((4, far, lanes)),
            dma((2, 4, far + 1, lanes)),
            dma((2, n - 1, cut)),
            dma((2, n - 1, cut)),
            dma((2, 2, n, cut)),
        ],
        compiler_params=pltpu.CompilerParams(
            collective_id=0, has_side_effects=True, vmem_limit_bytes=60 * 1024 * 1024
        ),
    )(
        saved_input,
        output_cotangent,
        recurrent_output,
        forget_logit,
        forget_cotangent,
        lower_bound.reshape(units // TILE, TILE),
        basis_in,
        basis_out,
        moment_in,
        second_in,
        moment_out,
        second_out,
        weight_in,
        weight_out.T,
    )
    blocks = 8 if model % 1024 == 0 else 1
    size = model // blocks
    outs = pl.pallas_call(
        settle,
        out_shape=(small, small, small, small, weight, weight, copied)
        + (jax.ShapeDtypeStruct((units, model), BF16),),
        in_specs=[hbm] * 8,
        out_specs=[hbm] * 8,
        scratch_shapes=[pltpu.VMEM((span, units), F32)] * 4
        + [pltpu.VMEM((depth, units), F32)] * 2
        + [
            pltpu.VMEM((2, blocks, size, units), BF16),
            pltpu.VMEM((units, model), BF16),
            dma((3, max(blocks, 6))),
            dma((3, max(blocks, 6))),
        ],
    )(*outs)
    return tuple(outs[:5]) + (outs[5].T, outs[6], outs[7])


def solution(mesh):
    return jax.shard_map(
        body,
        mesh=mesh,
        in_specs=(
            P("fs", None),
            P("fs", None),
            P("fs", "tp"),
            P("fs", "tp"),
            P("fs", "tp"),
            P("tp"),
            P("fs", None),
            P("fs", None),
            P("fs", "tp"),
            P("fs", "tp"),
            P("fs", "tp"),
            P("fs", "tp"),
            P("fs", "tp"),
            P("tp", "fs"),
        ),
        out_specs=(
            P("fs", "tp"),
            P("fs", "tp"),
            P("fs", "tp"),
            P("fs", "tp"),
            P("fs", "tp"),
            P("tp", "fs"),
            P(None, "tp"),
            P("tp", None),
        ),
        check_vma=False,
    )
```

```python
import functools

import jax
import jax.numpy as jnp
from jax import lax
from jax.experimental import pallas as pl
from jax.experimental.pallas import tpu as pltpu
from jax.sharding import PartitionSpec as P

MESH = pl.DeviceIdType.MESH
F32 = jnp.float32
BF16 = jnp.bfloat16
UNROLL = 16
TILE = 128


def loop(start, stop, body):
    if stop - start <= UNROLL:
        for i in range(start, stop):
            body(i)
    else:

        @pl.loop(start, stop)
        def _(i):
            body(i)


def mod(value, n):
    return lax.rem(value + 2 * n, n)


def kernel(
    nf,
    nt,
    limit,
    ahead,
    x_hbm,
    y_hbm,
    rec_hbm,
    logit_hbm,
    fcot_hbm,
    lower_ref,
    basis_in_hbm,
    basis_out_hbm,
    m_in,
    s_in,
    m_out,
    s_out,
    w_in,
    w_out,
    mn_in,
    sn_in,
    mn_out,
    sn_out,
    wn_in,
    wn_out,
    copy_in,
    copy_out,
    data,
    logit,
    fcot,
    cots,
    bas,
    own_bas,
    coded,
    term,
    part,
    peer,
    hop,
    step,
    flat,
    split,
    small,
    fresh,
    old,
    new,
    cp,
    tots,
    pre,
    lhs,
    load_sem,
    base_sem,
    out_sem,
    sem_a,
    ring_a,
    sem_b,
    ring_b,
    sum_sem,
    swap_sem,
    tot_sem,
    sem_d,
    ring_d,
    sem_f,
    ring_f,
    pair_f,
    sem_e,
    ring_e,
):
    f = lax.axis_index("fs")
    tp = lax.axis_index("tp")
    q = lax.rem(tp, 2)
    n = nf // 2
    z = n // 2
    core = lax.rem(f, 2)
    chip = f // 2
    row, column = chip // 2, lax.rem(chip, 2)
    me = (1 - column) * row + column * (n - 1 - row)
    partner = (f + 1 - 2 * core, tp)
    across = (f, tp + 1 - 2 * q)

    def chip_at(position):
        side = position // z
        return 2 * ((1 - side) * position + side * (n - 1 - position)) + side

    def dev_at(position):
        return chip_at(position) * 2 + core

    depth = basis_in_hbm.shape[0]
    half = depth // 2
    units = cots.shape[2]
    span = part.shape[2]
    lanes = 2 if units % 256 == 0 else 1
    width = units // lanes

    def own(ref, dev):
        return ref.at[pl.ds(pl.multiple_of(dev * depth, depth), depth)]

    def fetch(src, dst, i):
        return pltpu.make_async_copy(src, dst, load_sem.at[i])

    def pick(i, first, second, dst, sem):
        @pl.when(q == 0)
        def _():
            pltpu.make_async_copy(first, dst, sem).start()

        @pl.when(q == 1)
        def _():
            pltpu.make_async_copy(second, dst, sem).start()

        return pltpu.make_async_copy(first, dst, sem)

    own_load = pick(0, basis_in_hbm, basis_out_hbm, own(bas, f), base_sem.at[0])
    gate_loads = [fetch(logit_hbm, logit, 0), fetch(fcot_hbm, fcot, 1)]
    for copy in gate_loads:
        copy.start()
    data_load = pick(1, x_hbm, y_hbm, data, base_sem.at[1])
    late_loads = [
        fetch(src, dst, 2 + i)
        for i, (src, dst) in enumerate(
            (
                (rec_hbm, cots.at[1]),
                (m_in, small.at[0]),
                (s_in, small.at[1]),
                (m_out, small.at[2]),
                (s_out, small.at[3]),
                (basis_in_hbm, own_bas.at[0]),
                (basis_out_hbm, own_bas.at[1]),
                (w_in, old.at[0]),
                (w_out, old.at[1]),
            )
        )
    ]
    for copy in late_loads:
        copy.start()

    barrier = pltpu.get_barrier_semaphore()
    everyone = nf * nt
    my_id = f * nt + tp

    def other(i):
        target = lax.rem(my_id + i, everyone)
        return (target // nt, lax.rem(target, nt))

    @pl.loop(1, everyone)
    def _(i):
        pl.semaphore_signal(barrier, inc=1, device_id=other(i), device_id_type=MESH)

    pl.semaphore_wait(barrier, everyone - 1)

    far = n // 2
    near = n - 1 - far
    two_way = ((0, 1, far), (1, -1, far), (0, -1, near), (1, 1, near))

    def neighbour(way):
        return (dev_at(mod(me + way, n)), tp)

    def send(src, dst, sems, target):
        return pltpu.make_async_remote_copy(
            src_ref=src,
            dst_ref=dst,
            send_sem=sems[0],
            recv_sem=sems[1],
            device_id=target,
            device_id_type=MESH,
        )

    def arrive(ref, sem):
        pltpu.make_async_copy(ref, ref, sem).wait()

    def gather(view, chunks, sems, ring_sem, blocks, between=None):
        flows = two_way

        def remote(j, s, c, pair, target):
            t, way, _ = flows[j]
            block = view(t, dev_at(mod(me - way * s, n)), c)
            return send(block, block, pair, target)

        def ring_copy(j, s, c):
            pair = sems.at[0], ring_sem.at[j, s, c]
            return remote(j, s, c, pair, neighbour(flows[j][1]))

        def pair_copy(j, s, c):
            return remote(j, s, c, (sems.at[1], sems.at[2]), partner)

        def each(s, act):
            for c in range(chunks):
                for j in range(len(flows)):
                    act(j, s, c)

        def move(j, s, c, first=False, last=False):
            if not first:
                ring_copy(j, s - 1, c).wait_recv()
            if not last:
                ring_copy(j, s, c).start()
            if not first or j < 2:
                pair_copy(j, s, c).start()

        each(0, functools.partial(move, first=True))
        if between is not None:
            between()
        loop(1, near, lambda s: each(s, move))
        for s in range(near, far + 1):
            for c in range(chunks):
                for j, (_, _, hops) in enumerate(flows):
                    if s <= hops:
                        move(j, s, c, last=s == hops)
        arrive(blocks(n), sems.at[2])

        def finish():
            arrive(blocks(n), sems.at[1])
            arrive(blocks(n - 1), sems.at[0])

        return finish

    def make_gate():
        for copy in gate_loads:
            copy.wait()
        tile = 64

        @pl.loop(0, cots.shape[1] // tile)
        def _(i):
            at = pl.ds(pl.multiple_of(i * tile, tile), tile)
            for k in range(units // TILE):
                to = slice(k * TILE, (k + 1) * TILE)
                sig = jax.nn.sigmoid(logit[at, to].astype(F32))
                cots[0, at, to] = (
                    fcot[at, to].astype(F32)
                    * (1.0 - lower_ref[k : k + 1, :])
                    * sig
                    * (1.0 - sig)
                ).astype(BF16)

    ways = (1, -1)

    def ahead_copy(t, s):
        block = pre.at[t, chip_at(mod(me - ways[t] * s, n))]
        return send(block, block, (sem_e.at[0], ring_e.at[t, s]), neighbour(ways[t]))

    at_hop = [0]

    def advance():
        s = at_hop[0]
        if not ahead or s >= n:
            return
        for t in range(2):
            if s > 0:
                ahead_copy(t, s - 1).wait_recv()
            if s < n - 1:
                ahead_copy(t, s).start()
        at_hop[0] = s + 1

    def prepare():
        make_gate()
        for copy in late_loads[7:]:
            copy.wait()
        if ahead:
            for t in range(2):
                pre[t, chip] = old[t, :ahead].astype(BF16)

    own_load.wait()
    done_a = gather(
        lambda t, dev, c: bas.at[
            pl.ds(pl.multiple_of(dev * depth + t * half, half), half)
        ],
        1,
        sem_a,
        ring_a,
        lambda m: bas.at[pl.ds(0, m * depth)],
        prepare,
    )
    advance()
    data_load.wait()

    def piece(i):
        return pl.ds(pl.multiple_of(i * TILE, TILE), TILE)

    def swap(i):
        sems = swap_sem.at[0], swap_sem.at[1]
        return send(coded.at[0, piece(i)], coded.at[1, piece(i)], sems, across)

    tiles = data.shape[0] // TILE

    @pl.loop(0, tiles)
    def _(i):
        coded[0, piece(i)] = jnp.dot(
            data[piece(i)], bas[...], preferred_element_type=F32
        ).astype(BF16)
        swap(i).start()

    def lend(p):
        at = pl.multiple_of((2 * p + core) * depth, depth)
        return send(
            bas.at[pl.ds(at, ahead)],
            lhs.at[1, pl.ds(p * ahead, ahead)],
            (sem_e.at[1], sem_e.at[2]),
            across,
        )

    if ahead:
        for p in range(n):
            lend(p).start()

    def project(k):
        t = q if k == 0 else 1 - q
        for c in range(lanes):
            at = slice(c * width, (c + 1) * width)
            term[:, at] = lax.dot_general(
                coded[k], cots[t, :, at], (((0,), (0,)), ((), ())), preferred_element_type=F32
            )
        for i in range(nf):
            part[k * 2 + i % 2, i // 2] = term[i * span : (i + 1) * span]

    def pair_sum(k):
        sems = sum_sem.at[0, k], sum_sem.at[1, k]
        return send(part.at[k * 2 + 1 - core], peer.at[k], sems, partner)

    def ring_add(j, s, c):
        at = pl.ds(c * width, width)
        sems = sem_b.at[0], ring_b.at[j, s, c]
        return send(hop.at[j, s, :, at], hop.at[j, s + 1, :, at], sems, neighbour(two_way[j][1]))

    def mine(j, s, c):
        k, way, hops = two_way[j]
        at = pl.ds(c * width, width)
        place = chip_at(mod(me + way * (hops - s), n))
        return part[k * 2 + core, place, :, at] + peer[k, place, :, at]

    def begin(k):
        pair_sum(k).wait_recv()
        for c in range(lanes):
            at = pl.ds(c * width, width)
            for j in (k, k + 2):
                if two_way[j][2] > 0:
                    hop[j, 0, :, at] = mine(j, 0, c)
                    ring_add(j, 0, c).start()

    def relay(j, s, c):
        at = pl.ds(c * width, width)
        ring_add(j, s - 1, c).wait_recv()
        hop[j, s, :, at] = hop[j, s, :, at] + mine(j, s, c)
        ring_add(j, s, c).start()

    def relay_all(k, s):
        for c in range(lanes):
            for j in (k, k + 2):
                if isinstance(s, int) and s >= two_way[j][2]:
                    continue
                relay(j, s, c)

    def settle_sum(k):
        for c in range(lanes):
            at = pl.ds(c * width, width)
            ring_add(k + 2, near - 1, c).wait_recv()
            kept = hop[k + 2, near, :, at] + mine(k + 2, near, c)
            ring_add(k, far - 1, c).wait_recv()
            hop[k, far, :, at] = hop[k, far, :, at] + kept

    late_loads[0].wait()
    project(0)
    pair_sum(0).start()
    begin(0)
    advance()

    def relay_on(k, s):
        relay_all(k, s)
        advance()

    early = max(1, near - 1)
    loop(1, early, lambda s: relay_on(0, s))
    arrive(coded.at[1], swap_sem.at[1])
    project(1)
    pair_sum(1).start()
    advance()
    for s in range(early, far):
        relay_on(0, s)
    begin(1)
    settle_sum(0)
    loop(1, near, lambda s: relay_on(1, s))
    for s in range(near, far):
        relay_on(1, s)
    settle_sum(1)

    low = [hop[k, far] for k in range(2)]
    square = jnp.sum(low[0] * low[0] + low[1] * low[1], axis=(0, 1), keepdims=True)
    tots[my_id] = jnp.broadcast_to(square, tots.shape[1:])

    def tell(i):
        return send(tots.at[my_id], tots.at[my_id], (tot_sem.at[0], tot_sem.at[1]), other(i))

    @pl.loop(1, everyone)
    def _(i):
        tell(i).start()

    done_a()
    arrive(step.at[:, pl.ds(0, n - 1)], sem_b.at[0])
    for k in range(2):
        pair_sum(k).wait_send()
    arrive(coded.at[0], swap_sem.at[0])
    for copy in late_loads[1:7]:
        copy.wait()
    if ahead:
        arrive(lhs.at[1], sem_e.at[1])
        arrive(lhs.at[1], sem_e.at[2])
        for p in range(n):
            at = pl.multiple_of((2 * p + core) * depth, depth)
            lhs[0, p * ahead : (p + 1) * ahead] = bas[pl.ds(at, ahead)]
    all_tots = tots.at[pl.ds(0, everyone - 1)]
    arrive(all_tots, tot_sem.at[1])
    arrive(all_tots, tot_sem.at[0])

    total = jnp.sum(tots[...], axis=0)
    clip = jnp.minimum(1.0, jnp.sqrt(F32(limit)) * lax.rsqrt(total + 1e-06))[0:1, 0:1]
    for t in range(2):
        grad = clip * hop[lax.rem(q + t, 2), far]
        moment = 0.8 * small[2 * t] + 0.2 * grad
        second = 0.9 * small[2 * t + 1] + 0.1 * grad * grad
        fresh[2 * t] = moment
        fresh[2 * t + 1] = second
        step[t, f] = moment / (jnp.sqrt(second) + 1e-08)

    puts = [
        pltpu.make_async_copy(fresh.at[i], dst, out_sem.at[i])
        for i, dst in enumerate((mn_in, sn_in, mn_out, sn_out))
    ] + [
        pltpu.make_async_copy(new.at[t], dst, out_sem.at[4 + t])
        for t, dst in enumerate((wn_in, wn_out))
    ]

    for copy in puts[:4]:
        copy.start()
    done_d = gather(
        lambda t, dev, c: step.at[t, dev, :, pl.ds(c * width, width)],
        lanes,
        sem_d,
        ring_d,
        lambda m: step.at[:, pl.ds(0, m)],
    )

    cut = ring_f.shape[2]
    late = depth - ahead
    slab = late // cut

    def block(t, s, c):
        dev = dev_at(mod(me - ways[t] * s, n))
        return cp.at[t, pl.ds(pl.multiple_of(dev * depth + ahead + c * slab, 16), slab)]

    def pass_on(t, s, c):
        sems = sem_f.at[0], ring_f.at[t, s, c]
        return send(block(t, s, c), block(t, s, c), sems, neighbour(ways[t]))

    def share(t, s, c):
        sems = sem_f.at[1], pair_f.at[t, s]
        return send(block(t, s, c), block(t, s, c), sems, partner)

    outs = (copy_in, copy_out)

    def put(t, s):
        place = chip_at(mod(me - ways[t] * s, n))
        rows = pl.ds(pl.multiple_of(place * 2 * depth, 2 * depth), 2 * depth)
        return pltpu.make_async_copy(
            cp.at[t, rows], outs[t].at[rows], out_sem.at[6 + t]
        )

    rank = flat.shape[0]

    def apply(mat, steps):
        return jnp.dot(
            jnp.concatenate([mat, mat], axis=1), steps, preferred_element_type=F32
        )

    for t in range(2):
        for k in range(nf):
            flat[k * span : (k + 1) * span] = step[t, k]
        whole = flat[...]
        high = whole.astype(BF16)
        split[t, :rank] = high
        split[t, rank:] = (whole - high.astype(F32)).astype(BF16)
        made = old[t] - 0.01 * apply(own_bas[t], split[t])
        new[t] = made
        cp[t, pl.ds(pl.multiple_of(f * depth + ahead, 16), late)] = made[ahead:].astype(BF16)
        for c in range(cut):
            pass_on(t, 0, c).start()
        for c in range(cut):
            share(t, 0, c).start()
    for copy in puts[4:]:
        copy.start()

    def rows_of(t, p):
        at = pl.multiple_of((2 * p + core) * depth, depth)
        return cp.at[t, pl.ds(at, ahead)]

    if ahead:
        while at_hop[0] < n:
            advance()
        group = max(1, 256 // ahead)
        for k in range(2):
            t = q if k == 0 else 1 - q
            for p in range(0, n, group):
                size = min(group, n - p)
                moved = apply(lhs[k, p * ahead : (p + size) * ahead], split[t])
                for i in range(size):
                    kept = pre[t, p + i].astype(F32)
                    rows_of(t, p + i)[...] = (
                        kept - 0.01 * moved[i * ahead : (i + 1) * ahead]
                    ).astype(BF16)
                    send(
                        rows_of(t, p + i),
                        rows_of(t, p + i),
                        (sem_e.at[3], sem_e.at[4]),
                        partner,
                    ).start()
        arrive(pre, sem_e.at[4])

    def gone(s):
        for t in range(2):
            whole_block = cp.at[t, pl.ds(0, late)]
            arrive(whole_block, pair_f.at[t, s])
            put(t, s).start()

    def forward(s):
        for c in range(cut):
            for t in range(2):
                pass_on(t, s - 1, c).wait_recv()
                pass_on(t, s, c).start()
                share(t, s, c).start()
        gone(s - 1)

    loop(1, n - 1, forward)
    for c in range(cut):
        for t in range(2):
            pass_on(t, n - 2, c).wait_recv()
            share(t, n - 1, c).start()
    gone(n - 2)
    gone(n - 1)

    arrive(cp.at[:, pl.ds(0, (n - 1) * late)], sem_f.at[0])
    arrive(cp.at[:, pl.ds(0, n * late)], sem_f.at[1])
    if ahead:
        arrive(pre, sem_e.at[3])
        arrive(pre.at[:, pl.ds(0, n - 1)], sem_e.at[0])
    done_d()
    for copy in puts:
        copy.wait()
    for t in range(2):
        pltpu.make_async_copy(cp.at[t], outs[t], out_sem.at[6 + t]).wait()


def settle(*refs):
    ins, outs = refs[:8], refs[8:16]
    held, tall, wide, in_sem, out_sem = refs[16:22], refs[22], refs[23], refs[24], refs[25]
    blocks = tall.shape[1]
    size = tall.shape[2]

    def rows(i):
        return pl.ds(i * size, size)

    def get(t, i):
        return pltpu.make_async_copy(ins[6 + t].at[rows(i)], tall.at[t, i], in_sem.at[t, i])

    def put(t, i):
        if t == 0:
            return pltpu.make_async_copy(tall.at[0, i], outs[6].at[rows(i)], out_sem.at[0, i])
        return pltpu.make_async_copy(
            wide.at[:, rows(i)], outs[7].at[:, rows(i)], out_sem.at[1, i]
        )

    more = [
        (
            pltpu.make_async_copy(src, mid, in_sem.at[2, i]),
            pltpu.make_async_copy(mid, dst, out_sem.at[2, i]),
        )
        for i, (src, mid, dst) in enumerate(zip(ins[:6], held, outs[:6]))
    ]
    for i in range(blocks):
        for t in (1, 0):
            get(t, i).start()
    for load, _ in more:
        load.start()
    for i in range(blocks):
        get(1, i).wait()
        wide[:, rows(i)] = tall[1, i].T
        put(1, i).start()
        get(0, i).wait()
        put(0, i).start()
    for load, save in more:
        load.wait()
        save.start()
    for i in range(blocks):
        for t in (1, 0):
            put(t, i).wait()
    for _, save in more:
        save.wait()


def body(
    saved_input,
    output_cotangent,
    recurrent_output,
    forget_logit,
    forget_cotangent,
    lower_bound,
    basis_in,
    basis_out,
    moment_in,
    second_in,
    moment_out,
    second_out,
    weight_in,
    weight_out,
):
    nf, nt = lax.axis_size("fs"), lax.axis_size("tp")
    n = nf // 2
    tokens, model = saved_input.shape
    units = recurrent_output.shape[1]
    depth, rank = basis_in.shape
    span = moment_in.shape[0]
    limit = 2.0 * rank * units * nt
    small = jax.ShapeDtypeStruct((span, units), F32)
    weight = jax.ShapeDtypeStruct((depth, units), F32)
    copied = jax.ShapeDtypeStruct((model, units), BF16)
    cut = 2 if depth % 32 == 0 else 1
    lanes = 2 if units % 256 == 0 else 1
    far = n // 2
    ahead = depth // 3 // 16 * 16
    hbm = pl.BlockSpec(memory_space=pl.ANY)
    vmem = pl.BlockSpec(memory_space=pltpu.VMEM)
    dma = pltpu.SemaphoreType.DMA
    outs = pl.pallas_call(
        functools.partial(kernel, nf, nt, limit, ahead),
        out_shape=(small, small, small, small, weight, weight, copied, copied),
        in_specs=[hbm] * 5 + [vmem] + [hbm] * 8,
        out_specs=[hbm] * 8,
        scratch_shapes=[
            pltpu.VMEM((tokens, model), BF16),
            pltpu.VMEM((tokens, units), BF16),
            pltpu.VMEM((tokens, units), BF16),
            pltpu.VMEM((2, tokens, units), BF16),
            pltpu.VMEM((model, rank), BF16),
            pltpu.VMEM((2, depth, rank), BF16),
            pltpu.VMEM((2, tokens, rank), BF16),
            pltpu.VMEM((rank, units), F32),
            pltpu.VMEM((4, n, span, units), F32),
            pltpu.VMEM((2, n, span, units), F32),
            pltpu.VMEM((4, far + 1, span, units), F32),
            pltpu.VMEM((2, nf, span, units), F32),
            pltpu.VMEM((rank, units), F32),
            pltpu.VMEM((2, 2 * rank, units), BF16),
            pltpu.VMEM((4, span, units), F32),
            pltpu.VMEM((4, span, units), F32),
            pltpu.VMEM((2, depth, units), F32),
            pltpu.VMEM((2, depth, units), F32),
            pltpu.VMEM((2, model, units), BF16),
            pltpu.VMEM((nf * nt, 8, 128), F32),
            pltpu.VMEM((2, n, max(ahead, 16), units), BF16),
            pltpu.VMEM((2, n * max(ahead, 16), rank), BF16),
            dma((11,)),
            dma((2,)),
            dma((8,)),
            dma((3,)),
            dma((4, far, 1)),
            dma((1,)),
            dma((4, far, lanes)),
            dma((2, 2)),
            dma((2,)),
            dma((2,)),
            dma((3,)),
            dma((4, far, lanes)),
            dma((2,)),
            dma((2, n - 1, cut)),
            dma((2, n)),
            dma((5,)),
            dma((2, n - 1)),
        ],
        compiler_params=pltpu.CompilerParams(
            collective_id=0, has_side_effects=True, vmem_limit_bytes=60 * 1024 * 1024
        ),
    )(
        saved_input,
        output_cotangent,
        recurrent_output,
        forget_logit,
        forget_cotangent,
        lower_bound.reshape(units // TILE, TILE),
        basis_in,
        basis_out,
        moment_in,
        second_in,
        moment_out,
        second_out,
        weight_in,
        weight_out.T,
    )
    blocks = 8 if model % 1024 == 0 else 1
    size = model // blocks
    outs = pl.pallas_call(
        settle,
        out_shape=(small, small, small, small, weight, weight, copied)
        + (jax.ShapeDtypeStruct((units, model), BF16),),
        in_specs=[hbm] * 8,
        out_specs=[hbm] * 8,
        scratch_shapes=[pltpu.VMEM((span, units), F32)] * 4
        + [pltpu.VMEM((depth, units), F32)] * 2
        + [
            pltpu.VMEM((2, blocks, size, units), BF16),
            pltpu.VMEM((units, model), BF16),
            dma((3, max(blocks, 6))),
            dma((3, max(blocks, 6))),
        ],
    )(*outs)
    return tuple(outs[:5]) + (outs[5].T, outs[6], outs[7])


def solution(mesh):
    return jax.shard_map(
        body,
        mesh=mesh,
        in_specs=(
            P("fs", None),
            P("fs", None),
            P("fs", "tp"),
            P("fs", "tp"),
            P("fs", "tp"),
            P("tp"),
            P("fs", None),
            P("fs", None),
            P("fs", "tp"),
            P("fs", "tp"),
            P("fs", "tp"),
            P("fs", "tp"),
            P("fs", "tp"),
            P("tp", "fs"),
        ),
        out_specs=(
            P("fs", "tp"),
            P("fs", "tp"),
            P("fs", "tp"),
            P("fs", "tp"),
            P("fs", "tp"),
            P("tp", "fs"),
            P(None, "tp"),
            P("tp", None),
        ),
        check_vma=False,
    )
```

```python
import functools

import jax
import jax.numpy as jnp
from jax import lax
from jax.experimental import pallas as pl
from jax.experimental.pallas import tpu as pltpu
from jax.sharding import PartitionSpec as P

MESH = pl.DeviceIdType.MESH
F32 = jnp.float32
BF16 = jnp.bfloat16
UNROLL = 16
TILE = 128


def loop(start, stop, body):
    if stop - start <= UNROLL:
        for i in range(start, stop):
            body(i)
    else:

        @pl.loop(start, stop)
        def _(i):
            body(i)


def mod(value, n):
    return lax.rem(value + 2 * n, n)


def kernel(
    nf,
    nt,
    limit,
    ahead,
    x_hbm,
    y_hbm,
    rec_hbm,
    logit_hbm,
    fcot_hbm,
    lower_ref,
    basis_in_hbm,
    basis_out_hbm,
    m_in,
    s_in,
    m_out,
    s_out,
    w_in,
    w_out,
    fresh,
    new,
    cp,
    data,
    logit,
    fcot,
    cots,
    bas,
    own_bas,
    coded,
    term,
    part,
    peer,
    hop,
    step,
    flat,
    split,
    small,
    old,
    tots,
    pre,
    lhs,
    load_sem,
    base_sem,
    sem_a,
    ring_a,
    sem_b,
    ring_b,
    sum_sem,
    swap_sem,
    tot_sem,
    sem_d,
    ring_d,
    sem_f,
    ring_f,
    pair_f,
    sem_e,
    ring_e,
):
    f = lax.axis_index("fs")
    tp = lax.axis_index("tp")
    q = lax.rem(tp, 2)
    n = nf // 2
    z = n // 2
    core = lax.rem(f, 2)
    chip = f // 2
    row, column = chip // 2, lax.rem(chip, 2)
    me = (1 - column) * row + column * (n - 1 - row)
    partner = (f + 1 - 2 * core, tp)
    across = (f, tp + 1 - 2 * q)

    def chip_at(position):
        side = position // z
        return 2 * ((1 - side) * position + side * (n - 1 - position)) + side

    def dev_at(position):
        return chip_at(position) * 2 + core

    depth = basis_in_hbm.shape[0]
    half = depth // 2
    units = cots.shape[2]
    span = part.shape[2]
    lanes = 2 if units % 256 == 0 else 1
    width = units // lanes

    def own(ref, dev):
        return ref.at[pl.ds(pl.multiple_of(dev * depth, depth), depth)]

    def fetch(src, dst, i):
        return pltpu.make_async_copy(src, dst, load_sem.at[i])

    def pick(i, first, second, dst, sem):
        @pl.when(q == 0)
        def _():
            pltpu.make_async_copy(first, dst, sem).start()

        @pl.when(q == 1)
        def _():
            pltpu.make_async_copy(second, dst, sem).start()

        return pltpu.make_async_copy(first, dst, sem)

    own_load = pick(0, basis_in_hbm, basis_out_hbm, own(bas, f), base_sem.at[0])
    gate_loads = [fetch(logit_hbm, logit, 0), fetch(fcot_hbm, fcot, 1)]
    for copy in gate_loads:
        copy.start()
    data_load = pick(1, x_hbm, y_hbm, data, base_sem.at[1])
    late_loads = [
        fetch(src, dst, 2 + i)
        for i, (src, dst) in enumerate(
            (
                (rec_hbm, cots.at[1]),
                (m_in, small.at[0]),
                (s_in, small.at[1]),
                (m_out, small.at[2]),
                (s_out, small.at[3]),
                (basis_in_hbm, own_bas.at[0]),
                (basis_out_hbm, own_bas.at[1]),
                (w_in, old.at[0]),
                (w_out, old.at[1]),
            )
        )
    ]
    for copy in late_loads:
        copy.start()

    barrier = pltpu.get_barrier_semaphore()
    everyone = nf * nt
    my_id = f * nt + tp

    def other(i):
        target = lax.rem(my_id + i, everyone)
        return (target // nt, lax.rem(target, nt))

    @pl.loop(1, everyone)
    def _(i):
        pl.semaphore_signal(barrier, inc=1, device_id=other(i), device_id_type=MESH)

    pl.semaphore_wait(barrier, everyone - 1)

    far = n // 2
    near = n - 1 - far
    two_way = ((0, 1, far), (1, -1, far), (0, -1, near), (1, 1, near))

    def neighbour(way):
        return (dev_at(mod(me + way, n)), tp)

    def send(src, dst, sems, target):
        return pltpu.make_async_remote_copy(
            src_ref=src,
            dst_ref=dst,
            send_sem=sems[0],
            recv_sem=sems[1],
            device_id=target,
            device_id_type=MESH,
        )

    def arrive(ref, sem):
        pltpu.make_async_copy(ref, ref, sem).wait()

    def gather(view, chunks, sems, ring_sem, blocks, between=None, after=None):
        flows = two_way

        def remote(j, s, c, pair, target):
            t, way, _ = flows[j]
            block = view(t, dev_at(mod(me - way * s, n)), c)
            return send(block, block, pair, target)

        def ring_copy(j, s, c):
            pair = sems.at[0], ring_sem.at[j, s, c]
            return remote(j, s, c, pair, neighbour(flows[j][1]))

        def pair_copy(j, s, c):
            return remote(j, s, c, (sems.at[1], sems.at[2]), partner)

        def each(s, act):
            for c in range(chunks):
                for j in range(len(flows)):
                    act(j, s, c)

        def move(j, s, c, first=False, last=False):
            if not first:
                ring_copy(j, s - 1, c).wait_recv()
            if not last:
                ring_copy(j, s, c).start()
            if not first or j < 2:
                pair_copy(j, s, c).start()

        each(0, functools.partial(move, first=True))
        if between is not None:
            between()
        loop(1, near, lambda s: each(s, move))
        for s in range(near, far + 1):
            for c in range(chunks):
                for j, (_, _, hops) in enumerate(flows):
                    if s <= hops:
                        move(j, s, c, last=s == hops)
        if after is not None:
            after()
        arrive(blocks(n), sems.at[2])

        def finish():
            arrive(blocks(n), sems.at[1])
            arrive(blocks(n - 1), sems.at[0])

        return finish

    def make_gate():
        for copy in gate_loads:
            copy.wait()
        tile = 64

        @pl.loop(0, cots.shape[1] // tile)
        def _(i):
            at = pl.ds(pl.multiple_of(i * tile, tile), tile)
            for k in range(units // TILE):
                to = slice(k * TILE, (k + 1) * TILE)
                sig = jax.nn.sigmoid(logit[at, to].astype(F32))
                cots[0, at, to] = (
                    fcot[at, to].astype(F32)
                    * (1.0 - lower_ref[k : k + 1, :])
                    * sig
                    * (1.0 - sig)
                ).astype(BF16)

    ways = (1, -1)

    def ahead_copy(t, s):
        block = pre.at[t, chip_at(mod(me - ways[t] * s, n))]
        return send(block, block, (sem_e.at[0], ring_e.at[t, s]), neighbour(ways[t]))

    at_hop = [0]

    def advance():
        s = at_hop[0]
        if not ahead or s >= n:
            return
        for t in range(2):
            if s > 0:
                ahead_copy(t, s - 1).wait_recv()
            if s < n - 1:
                ahead_copy(t, s).start()
        at_hop[0] = s + 1

    def prepare():
        make_gate()
        for copy in late_loads[7:]:
            copy.wait()
        if ahead:
            for t in range(2):
                pre[t, chip] = old[t, :ahead].astype(BF16)

    own_load.wait()
    done_a = gather(
        lambda t, dev, c: bas.at[
            pl.ds(pl.multiple_of(dev * depth + t * half, half), half)
        ],
        1,
        sem_a,
        ring_a,
        lambda m: bas.at[pl.ds(0, m * depth)],
        prepare,
        advance,
    )
    data_load.wait()

    def piece(i):
        return pl.ds(pl.multiple_of(i * TILE, TILE), TILE)

    def swap(i):
        sems = swap_sem.at[0], swap_sem.at[1]
        return send(coded.at[0, piece(i)], coded.at[1, piece(i)], sems, across)

    tiles = data.shape[0] // TILE

    @pl.loop(0, tiles)
    def _(i):
        coded[0, piece(i)] = jnp.dot(
            data[piece(i)], bas[...], preferred_element_type=F32
        ).astype(BF16)
        swap(i).start()

    def lend(p):
        at = pl.multiple_of((2 * p + core) * depth, depth)
        return send(
            bas.at[pl.ds(at, ahead)],
            lhs.at[1, pl.ds(p * ahead, ahead)],
            (sem_e.at[1], sem_e.at[2]),
            across,
        )

    if ahead:
        for p in range(n):
            lend(p).start()

    def project(k):
        t = q if k == 0 else 1 - q
        for c in range(lanes):
            at = slice(c * width, (c + 1) * width)
            term[:, at] = lax.dot_general(
                coded[k], cots[t, :, at], (((0,), (0,)), ((), ())), preferred_element_type=F32
            )
        for i in range(nf):
            part[k * 2 + i % 2, i // 2] = term[i * span : (i + 1) * span]

    def pair_sum(k):
        sems = sum_sem.at[0, k], sum_sem.at[1, k]
        return send(part.at[k * 2 + 1 - core], peer.at[k], sems, partner)

    def ring_add(j, s, c):
        at = pl.ds(c * width, width)
        sems = sem_b.at[0], ring_b.at[j, s, c]
        return send(hop.at[j, s, :, at], hop.at[j, s + 1, :, at], sems, neighbour(two_way[j][1]))

    def mine(j, s, c):
        k, way, hops = two_way[j]
        at = pl.ds(c * width, width)
        place = chip_at(mod(me + way * (hops - s), n))
        return part[k * 2 + core, place, :, at] + peer[k, place, :, at]

    def begin(k):
        pair_sum(k).wait_recv()
        for c in range(lanes):
            at = pl.ds(c * width, width)
            for j in (k, k + 2):
                if two_way[j][2] > 0:
                    hop[j, 0, :, at] = mine(j, 0, c)
                    ring_add(j, 0, c).start()

    def relay(j, s, c):
        at = pl.ds(c * width, width)
        ring_add(j, s - 1, c).wait_recv()
        hop[j, s, :, at] = hop[j, s, :, at] + mine(j, s, c)
        ring_add(j, s, c).start()

    def relay_all(k, s):
        for c in range(lanes):
            for j in (k, k + 2):
                if isinstance(s, int) and s >= two_way[j][2]:
                    continue
                relay(j, s, c)

    def settle_sum(k):
        for c in range(lanes):
            at = pl.ds(c * width, width)
            ring_add(k + 2, near - 1, c).wait_recv()
            kept = hop[k + 2, near, :, at] + mine(k + 2, near, c)
            ring_add(k, far - 1, c).wait_recv()
            hop[k, far, :, at] = hop[k, far, :, at] + kept

    late_loads[0].wait()
    project(0)
    pair_sum(0).start()
    advance()
    begin(0)
    early = max(1, near - 1)
    loop(1, early, lambda s: relay_all(0, s))
    advance()
    arrive(coded.at[1], swap_sem.at[1])
    project(1)
    pair_sum(1).start()
    loop(early, near, lambda s: relay_all(0, s))
    begin(1)
    advance()
    for s in range(near, far):
        relay_all(0, s)
    loop(1, near, lambda s: relay_all(1, s))
    advance()
    settle_sum(0)
    for s in range(near, far):
        relay_all(1, s)
    settle_sum(1)

    low = [hop[k, far] for k in range(2)]
    square = jnp.sum(low[0] * low[0] + low[1] * low[1], axis=(0, 1), keepdims=True)
    tots[my_id] = jnp.broadcast_to(square, tots.shape[1:])

    def tell(i):
        return send(tots.at[my_id], tots.at[my_id], (tot_sem.at[0], tot_sem.at[1]), other(i))

    @pl.loop(1, everyone)
    def _(i):
        tell(i).start()

    advance()

    done_a()
    arrive(step.at[:, pl.ds(0, n - 1)], sem_b.at[0])
    for k in range(2):
        pair_sum(k).wait_send()
    arrive(coded.at[0], swap_sem.at[0])
    for copy in late_loads[1:7]:
        copy.wait()
    if ahead:
        arrive(lhs.at[1], sem_e.at[1])
        arrive(lhs.at[1], sem_e.at[2])
        for p in range(n):
            at = pl.multiple_of((2 * p + core) * depth, depth)
            lhs[0, p * ahead : (p + 1) * ahead] = bas[pl.ds(at, ahead)]
    all_tots = tots.at[pl.ds(0, everyone - 1)]
    arrive(all_tots, tot_sem.at[1])
    arrive(all_tots, tot_sem.at[0])

    total = jnp.sum(tots[...], axis=0)
    clip = jnp.minimum(1.0, jnp.sqrt(F32(limit)) * lax.rsqrt(total + 1e-06))[0:1, 0:1]
    for t in range(2):
        grad = clip * hop[lax.rem(q + t, 2), far]
        moment = 0.8 * small[2 * t] + 0.2 * grad
        second = 0.9 * small[2 * t + 1] + 0.1 * grad * grad
        fresh[2 * t] = moment
        fresh[2 * t + 1] = second
        step[t, f] = moment / (jnp.sqrt(second) + 1e-08)

    done_d = gather(
        lambda t, dev, c: step.at[t, dev, :, pl.ds(c * width, width)],
        lanes,
        sem_d,
        ring_d,
        lambda m: step.at[:, pl.ds(0, m)],
        None,
        advance,
    )

    cut = ring_f.shape[2]
    late = depth - ahead
    slab = late // cut

    def block(t, s, c):
        dev = dev_at(mod(me - ways[t] * s, n))
        return cp.at[t, pl.ds(pl.multiple_of(dev * depth + ahead + c * slab, 16), slab)]

    def pass_on(t, s, c):
        sems = sem_f.at[0], ring_f.at[t, s, c]
        return send(block(t, s, c), block(t, s, c), sems, neighbour(ways[t]))

    def share(t, s, c):
        sems = sem_f.at[1], pair_f.at[t, s]
        return send(block(t, s, c), block(t, s, c), sems, partner)

    rank = flat.shape[0]

    def apply(mat, steps):
        return jnp.dot(
            jnp.concatenate([mat, mat], axis=1), steps, preferred_element_type=F32
        )

    for t in range(2):
        for k in range(nf):
            flat[k * span : (k + 1) * span] = step[t, k]
        whole = flat[...]
        high = whole.astype(BF16)
        split[t, :rank] = high
        split[t, rank:] = (whole - high.astype(F32)).astype(BF16)
        made = old[t] - 0.01 * apply(own_bas[t], split[t])
        new[t] = made
        cp[t, pl.ds(pl.multiple_of(f * depth + ahead, 16), late)] = made[ahead:].astype(BF16)
        for c in range(cut):
            pass_on(t, 0, c).start()
        for c in range(cut):
            share(t, 0, c).start()
    def rows_of(t, p):
        at = pl.multiple_of((2 * p + core) * depth, depth)
        return cp.at[t, pl.ds(at, ahead)]

    if ahead:
        while at_hop[0] < n:
            advance()
        group = max(1, 256 // ahead)
        for k in range(2):
            t = q if k == 0 else 1 - q
            for p in range(0, n, group):
                size = min(group, n - p)
                moved = apply(lhs[k, p * ahead : (p + size) * ahead], split[t])
                for i in range(size):
                    kept = pre[t, p + i].astype(F32)
                    rows_of(t, p + i)[...] = (
                        kept - 0.01 * moved[i * ahead : (i + 1) * ahead]
                    ).astype(BF16)
                    send(
                        rows_of(t, p + i),
                        rows_of(t, p + i),
                        (sem_e.at[3], sem_e.at[4]),
                        partner,
                    ).start()
        arrive(pre, sem_e.at[4])

    def gone(s):
        for t in range(2):
            whole_block = cp.at[t, pl.ds(0, late)]
            arrive(whole_block, pair_f.at[t, s])

    def forward(s):
        for c in range(cut):
            for t in range(2):
                pass_on(t, s - 1, c).wait_recv()
                pass_on(t, s, c).start()
                share(t, s, c).start()
        gone(s - 1)

    loop(1, n - 1, forward)
    for c in range(cut):
        for t in range(2):
            pass_on(t, n - 2, c).wait_recv()
            share(t, n - 1, c).start()
    gone(n - 2)
    gone(n - 1)

    arrive(cp.at[:, pl.ds(0, (n - 1) * late)], sem_f.at[0])
    arrive(cp.at[:, pl.ds(0, n * late)], sem_f.at[1])
    if ahead:
        arrive(pre, sem_e.at[3])
        arrive(pre.at[:, pl.ds(0, n - 1)], sem_e.at[0])
    done_d()


def settle(fresh, new, cp, *refs):
    outs, wide, sem = refs[:8], refs[8], refs[9]
    model = cp.shape[1]
    size = sem.shape[0]
    blocks = size - 8
    step = model // blocks
    saves = [
        pltpu.make_async_copy(src, dst, sem.at[blocks + i])
        for i, (src, dst) in enumerate(
            [(fresh.at[i], outs[i]) for i in range(4)]
            + [(new.at[i], outs[4 + i]) for i in range(2)]
            + [(cp.at[0], outs[6])]
        )
    ]
    saves = saves[::-1]
    for save in saves:
        save.start()
    for i in range(blocks):
        at = pl.ds(i * step, step)
        wide[:, at] = cp[1, at].T
        saves.append(pltpu.make_async_copy(wide.at[:, at], outs[7].at[:, at], sem.at[i]))
        saves[-1].start()
    for save in saves:
        save.wait()


def body(
    saved_input,
    output_cotangent,
    recurrent_output,
    forget_logit,
    forget_cotangent,
    lower_bound,
    basis_in,
    basis_out,
    moment_in,
    second_in,
    moment_out,
    second_out,
    weight_in,
    weight_out,
):
    nf, nt = lax.axis_size("fs"), lax.axis_size("tp")
    n = nf // 2
    tokens, model = saved_input.shape
    units = recurrent_output.shape[1]
    depth, rank = basis_in.shape
    span = moment_in.shape[0]
    limit = 2.0 * rank * units * nt
    small = jax.ShapeDtypeStruct((span, units), F32)
    weight = jax.ShapeDtypeStruct((depth, units), F32)
    copied = jax.ShapeDtypeStruct((model, units), BF16)
    held = (
        jax.ShapeDtypeStruct((4, span, units), F32),
        jax.ShapeDtypeStruct((2, depth, units), F32),
        jax.ShapeDtypeStruct((2, model, units), BF16),
    )
    cut = 2 if depth % 32 == 0 else 1
    lanes = 2 if units % 256 == 0 else 1
    far = n // 2
    ahead = depth // 3 // 16 * 16
    hbm = pl.BlockSpec(memory_space=pltpu.HBM)
    vmem = pl.BlockSpec(memory_space=pltpu.VMEM)
    dma = pltpu.SemaphoreType.DMA
    outs = pl.pallas_call(
        functools.partial(kernel, nf, nt, limit, ahead),
        out_shape=tuple(pltpu.VMEM(o.shape, o.dtype) for o in held),
        in_specs=[hbm] * 5 + [vmem] + [hbm] * 8,
        out_specs=[vmem] * 3,
        scratch_shapes=[
            pltpu.VMEM((tokens, model), BF16),
            pltpu.VMEM((tokens, units), BF16),
            pltpu.VMEM((tokens, units), BF16),
            pltpu.VMEM((2, tokens, units), BF16),
            pltpu.VMEM((model, rank), BF16),
            pltpu.VMEM((2, depth, rank), BF16),
            pltpu.VMEM((2, tokens, rank), BF16),
            pltpu.VMEM((rank, units), F32),
            pltpu.VMEM((4, n, span, units), F32),
            pltpu.VMEM((2, n, span, units), F32),
            pltpu.VMEM((4, far + 1, span, units), F32),
            pltpu.VMEM((2, nf, span, units), F32),
            pltpu.VMEM((rank, units), F32),
            pltpu.VMEM((2, 2 * rank, units), BF16),
            pltpu.VMEM((4, span, units), F32),
            pltpu.VMEM((2, depth, units), F32),
            pltpu.VMEM((nf * nt, 8, 128), F32),
            pltpu.VMEM((2, n, max(ahead, 16), units), BF16),
            pltpu.VMEM((2, n * max(ahead, 16), rank), BF16),
            dma((11,)),
            dma((2,)),
            dma((3,)),
            dma((4, far, 1)),
            dma((1,)),
            dma((4, far, lanes)),
            dma((2, 2)),
            dma((2,)),
            dma((2,)),
            dma((3,)),
            dma((4, far, lanes)),
            dma((2,)),
            dma((2, n - 1, cut)),
            dma((2, n)),
            dma((5,)),
            dma((2, n - 1)),
        ],
        compiler_params=pltpu.CompilerParams(
            collective_id=0, has_side_effects=True, vmem_limit_bytes=50 * 1024 * 1024
        ),
    )(
        saved_input,
        output_cotangent,
        recurrent_output,
        forget_logit,
        forget_cotangent,
        lower_bound.reshape(units // TILE, TILE),
        basis_in,
        basis_out,
        moment_in,
        second_in,
        moment_out,
        second_out,
        weight_in,
        weight_out.T,
    )
    blocks = 8 if model % 1024 == 0 else 1
    outs = pl.pallas_call(
        settle,
        out_shape=(small, small, small, small, weight, weight, copied)
        + (jax.ShapeDtypeStruct((units, model), BF16),),
        in_specs=[vmem] * 3,
        out_specs=[hbm] * 8,
        scratch_shapes=[pltpu.VMEM((units, model), BF16), dma((blocks + 8,))],
        compiler_params=pltpu.CompilerParams(vmem_limit_bytes=40 * 1024 * 1024),
    )(*outs)
    return tuple(outs[:5]) + (outs[5].T, outs[6], outs[7])


def solution(mesh):
    return jax.shard_map(
        body,
        mesh=mesh,
        in_specs=(
            P("fs", None),
            P("fs", None),
            P("fs", "tp"),
            P("fs", "tp"),
            P("fs", "tp"),
            P("tp"),
            P("fs", None),
            P("fs", None),
            P("fs", "tp"),
            P("fs", "tp"),
            P("fs", "tp"),
            P("fs", "tp"),
            P("fs", "tp"),
            P("tp", "fs"),
        ),
        out_specs=(
            P("fs", "tp"),
            P("fs", "tp"),
            P("fs", "tp"),
            P("fs", "tp"),
            P("fs", "tp"),
            P("tp", "fs"),
            P(None, "tp"),
            P("tp", None),
        ),
        check_vma=False,
    )
```

```python
import functools

import jax
import jax.numpy as jnp
from jax import lax
from jax.experimental import pallas as pl
from jax.experimental.pallas import tpu as pltpu
from jax.sharding import PartitionSpec as P

MESH = pl.DeviceIdType.MESH
F32 = jnp.float32
BF16 = jnp.bfloat16
UNROLL = 16
TILE = 128


def loop(start, stop, body):
    if stop - start <= UNROLL:
        for i in range(start, stop):
            body(i)
    else:

        @pl.loop(start, stop)
        def _(i):
            body(i)


def mod(value, n):
    return lax.rem(value + 2 * n, n)


def kernel(
    nf,
    nt,
    limit,
    ahead,
    x_hbm,
    y_hbm,
    rec_hbm,
    logit_hbm,
    fcot_hbm,
    lower_ref,
    basis_in_hbm,
    basis_out_hbm,
    m_in,
    s_in,
    m_out,
    s_out,
    w_in,
    w_out,
    fresh,
    new,
    cp,
    data,
    logit,
    fcot,
    cots,
    bas,
    own_bas,
    coded,
    term,
    part,
    peer,
    hop,
    lead,
    low,
    step,
    flat,
    split,
    small,
    old,
    tots,
    pre,
    lhs,
    load_sem,
    base_sem,
    sem_a,
    ring_a,
    sem_b,
    ring_b,
    sum_sem,
    swap_sem,
    tot_sem,
    sem_d,
    ring_d,
    sem_f,
    ring_f,
    pair_f,
    sem_e,
    ring_e,
):
    f = lax.axis_index("fs")
    tp = lax.axis_index("tp")
    q = lax.rem(tp, 2)
    n = nf // 2
    z = n // 2
    core = lax.rem(f, 2)
    chip = f // 2
    row, column = chip // 2, lax.rem(chip, 2)
    me = (1 - column) * row + column * (n - 1 - row)
    partner = (f + 1 - 2 * core, tp)
    across = (f, tp + 1 - 2 * q)

    def chip_at(position):
        side = position // z
        return 2 * ((1 - side) * position + side * (n - 1 - position)) + side

    def dev_at(position):
        return chip_at(position) * 2 + core

    depth = basis_in_hbm.shape[0]
    half = depth // 2
    units = cots.shape[2]
    span = part.shape[2]
    lanes = 2 if units % 256 == 0 else 1
    width = units // lanes

    def own(ref, dev):
        return ref.at[pl.ds(pl.multiple_of(dev * depth, depth), depth)]

    def fetch(src, dst, i):
        return pltpu.make_async_copy(src, dst, load_sem.at[i])

    def pick(i, first, second, dst, sem):
        @pl.when(q == 0)
        def _():
            pltpu.make_async_copy(first, dst, sem).start()

        @pl.when(q == 1)
        def _():
            pltpu.make_async_copy(second, dst, sem).start()

        return pltpu.make_async_copy(first, dst, sem)

    own_load = pick(0, basis_in_hbm, basis_out_hbm, own(bas, f), base_sem.at[0])
    gate_loads = [fetch(logit_hbm, logit, 0), fetch(fcot_hbm, fcot, 1)]
    for copy in gate_loads:
        copy.start()
    data_load = pick(1, x_hbm, y_hbm, data, base_sem.at[1])
    late_loads = [
        fetch(src, dst, 2 + i)
        for i, (src, dst) in enumerate(
            (
                (rec_hbm, cots.at[1]),
                (m_in, small.at[0]),
                (s_in, small.at[1]),
                (m_out, small.at[2]),
                (s_out, small.at[3]),
                (basis_in_hbm, own_bas.at[0]),
                (basis_out_hbm, own_bas.at[1]),
                (w_in, old.at[0]),
                (w_out, old.at[1]),
            )
        )
    ]
    for copy in late_loads:
        copy.start()

    barrier = pltpu.get_barrier_semaphore()
    everyone = nf * nt
    my_id = f * nt + tp

    def other(i):
        target = lax.rem(my_id + i, everyone)
        return (target // nt, lax.rem(target, nt))

    far = n // 2
    near = n - 1 - far
    two_way = ((0, 1, far), (1, -1, far), (0, -1, near), (1, 1, near))

    def neighbour(way):
        return (dev_at(mod(me + way, n)), tp)

    for target in (neighbour(1), neighbour(-1), partner, across):
        pl.semaphore_signal(barrier, inc=1, device_id=target, device_id_type=MESH)
    pl.semaphore_wait(barrier, 4)

    def send(src, dst, sems, target):
        return pltpu.make_async_remote_copy(
            src_ref=src,
            dst_ref=dst,
            send_sem=sems[0],
            recv_sem=sems[1],
            device_id=target,
            device_id_type=MESH,
        )

    def arrive(ref, sem):
        pltpu.make_async_copy(ref, ref, sem).wait()

    def gather(view, chunks, sems, ring_sem, blocks, between=None, after=None):
        flows = two_way

        def remote(j, s, c, pair, target):
            t, way, _ = flows[j]
            block = view(t, dev_at(mod(me - way * s, n)), c)
            return send(block, block, pair, target)

        def ring_copy(j, s, c):
            pair = sems.at[0], ring_sem.at[j, s, c]
            return remote(j, s, c, pair, neighbour(flows[j][1]))

        def pair_copy(j, s, c):
            return remote(j, s, c, (sems.at[1], sems.at[2]), partner)

        def each(s, act):
            for c in range(chunks):
                for j in range(len(flows)):
                    act(j, s, c)

        def move(j, s, c, first=False, last=False):
            if not first:
                ring_copy(j, s - 1, c).wait_recv()
            if not last:
                ring_copy(j, s, c).start()
            if not first or j < 2:
                pair_copy(j, s, c).start()

        each(0, functools.partial(move, first=True))
        if between is not None:
            between()
        loop(1, near, lambda s: each(s, move))
        for s in range(near, far + 1):
            for c in range(chunks):
                for j, (_, _, hops) in enumerate(flows):
                    if s <= hops:
                        move(j, s, c, last=s == hops)
        if after is not None:
            after()
        arrive(blocks(n), sems.at[2])

        def finish():
            arrive(blocks(n), sems.at[1])
            arrive(blocks(n - 1), sems.at[0])

        return finish

    def make_gate():
        for copy in gate_loads:
            copy.wait()
        tile = 64

        @pl.loop(0, cots.shape[1] // tile)
        def _(i):
            at = pl.ds(pl.multiple_of(i * tile, tile), tile)
            for k in range(units // TILE):
                to = slice(k * TILE, (k + 1) * TILE)
                sig = jax.nn.sigmoid(logit[at, to].astype(F32))
                cots[0, at, to] = (
                    fcot[at, to].astype(F32)
                    * (1.0 - lower_ref[k : k + 1, :])
                    * sig
                    * (1.0 - sig)
                ).astype(BF16)

    ways = (1, -1)

    def ahead_copy(t, s):
        block = pre.at[t, chip_at(mod(me - ways[t] * s, n))]
        return send(block, block, (sem_e.at[0], ring_e.at[t, s]), neighbour(ways[t]))

    at_hop = [0]

    def advance():
        s = at_hop[0]
        if not ahead or s >= n:
            return
        for t in range(2):
            if s > 0:
                ahead_copy(t, s - 1).wait_recv()
            if s < n - 1:
                ahead_copy(t, s).start()
        at_hop[0] = s + 1

    def prepare():
        make_gate()
        for copy in late_loads[7:]:
            copy.wait()
        if ahead:
            for t in range(2):
                pre[t, chip] = old[t, :ahead].astype(BF16)

    own_load.wait()
    done_a = gather(
        lambda t, dev, c: bas.at[
            pl.ds(pl.multiple_of(dev * depth + t * half, half), half)
        ],
        1,
        sem_a,
        ring_a,
        lambda m: bas.at[pl.ds(0, m * depth)],
        prepare,
        advance,
    )
    data_load.wait()

    def piece(i):
        return pl.ds(pl.multiple_of(i * TILE, TILE), TILE)

    def swap(i):
        sems = swap_sem.at[0], swap_sem.at[1]
        return send(coded.at[0, piece(i)], coded.at[1, piece(i)], sems, across)

    tiles = data.shape[0] // TILE

    @pl.loop(0, tiles)
    def _(i):
        coded[0, piece(i)] = jnp.dot(
            data[piece(i)], bas[...], preferred_element_type=F32
        ).astype(BF16)
        swap(i).start()

    def lend(p):
        at = pl.multiple_of((2 * p + core) * depth, depth)
        return send(
            bas.at[pl.ds(at, ahead)],
            lhs.at[1, pl.ds(p * ahead, ahead)],
            (sem_e.at[1], sem_e.at[2]),
            across,
        )

    if ahead:
        for p in range(n):
            lend(p).start()

    def project(k):
        t = q if k == 0 else 1 - q
        for c in range(lanes):
            at = slice(c * width, (c + 1) * width)
            term[:, at] = lax.dot_general(
                coded[k], cots[t, :, at], (((0,), (0,)), ((), ())), preferred_element_type=F32
            )
        for i in range(nf):
            part[k * 2 + i % 2, i // 2] = term[i * span : (i + 1) * span]

    def place_of(j, s):
        _, way, hops = two_way[j]
        return chip_at(mod(me + way * (hops - s), n))

    def pair_sum(k):
        def group(s):
            for j in (k, k + 2):
                if not isinstance(s, int) or s < two_way[j][2] or (s == far and j == k):
                    place = place_of(j, s)
                    sems = sum_sem.at[0, 0], sum_sem.at[1 + k, s]
                    send(
                        part.at[k * 2 + 1 - core, place], peer.at[k, place], sems, partner
                    ).start()

        loop(0, near, group)
        for s in range(near, far + 1):
            group(s)

    def paired(k, s):
        count = 2 if not isinstance(s, int) or s < near else 1
        arrive(peer.at[k, pl.ds(0, count)], sum_sem.at[1 + k, s])

    def ring_add(j, s, c):
        at = pl.ds(c * width, width)
        sems = sem_b.at[0], ring_b.at[j, s, c]
        return send(lead.at[j, s, :, at], hop.at[j, s, :, at], sems, neighbour(two_way[j][1]))

    def mine(j, s, c):
        k = two_way[j][0]
        at = pl.ds(c * width, width)
        place = place_of(j, s)
        return part[k * 2 + core, place, :, at] + peer[k, place, :, at]

    def begin(k):
        paired(k, 0)
        for c in range(lanes):
            at = pl.ds(c * width, width)
            for j in (k, k + 2):
                if two_way[j][2] > 0:
                    lead[j, 0, :, at] = mine(j, 0, c).astype(lead.dtype)
                    ring_add(j, 0, c).start()

    def relay(j, s, c):
        at = pl.ds(c * width, width)
        ring_add(j, s - 1, c).wait_recv()
        lead[j, s, :, at] = (hop[j, s - 1, :, at].astype(F32) + mine(j, s, c)).astype(
            lead.dtype
        )
        ring_add(j, s, c).start()

    def relay_all(k, s):
        paired(k, s)
        for c in range(lanes):
            for j in (k, k + 2):
                if isinstance(s, int) and s >= two_way[j][2]:
                    continue
                relay(j, s, c)

    def settle_sum(k):
        paired(k, far)
        for c in range(lanes):
            at = pl.ds(c * width, width)
            ring_add(k + 2, near - 1, c).wait_recv()
            kept = hop[k + 2, near - 1, :, at].astype(F32) + mine(k + 2, near, c)
            ring_add(k, far - 1, c).wait_recv()
            low[k, :, at] = hop[k, far - 1, :, at].astype(F32) + kept

    late_loads[0].wait()
    project(0)
    pair_sum(0)
    advance()
    begin(0)
    early = max(1, near - 1)
    loop(1, early, lambda s: relay_all(0, s))
    advance()
    arrive(coded.at[1], swap_sem.at[1])
    project(1)
    pair_sum(1)
    loop(early, near, lambda s: relay_all(0, s))
    begin(1)
    advance()
    for s in range(near, far):
        relay_all(0, s)
    loop(1, near, lambda s: relay_all(1, s))
    advance()
    settle_sum(0)
    for s in range(near, far):
        relay_all(1, s)
    settle_sum(1)

    square = jnp.sum(low[0] * low[0] + low[1] * low[1], axis=(0, 1), keepdims=True)
    tots[my_id] = jnp.broadcast_to(square, tots.shape[1:])

    def tell(i):
        return send(tots.at[my_id], tots.at[my_id], (tot_sem.at[0], tot_sem.at[1]), other(i))

    @pl.loop(1, everyone)
    def _(i):
        tell(i).start()

    advance()

    done_a()
    arrive(lead.at[pl.ds(0, 2)], sem_b.at[0])
    arrive(lead.at[pl.ds(0, 2), pl.ds(0, near)], sem_b.at[0])
    arrive(peer, sum_sem.at[0, 0])
    arrive(coded.at[0], swap_sem.at[0])
    for copy in late_loads[1:7]:
        copy.wait()
    if ahead:
        arrive(lhs.at[1], sem_e.at[1])
        arrive(lhs.at[1], sem_e.at[2])
        for p in range(n):
            at = pl.multiple_of((2 * p + core) * depth, depth)
            lhs[0, p * ahead : (p + 1) * ahead] = bas[pl.ds(at, ahead)]
    all_tots = tots.at[pl.ds(0, everyone - 1)]
    arrive(all_tots, tot_sem.at[1])
    arrive(all_tots, tot_sem.at[0])

    total = jnp.sum(tots[...], axis=0)
    clip = jnp.minimum(1.0, jnp.sqrt(F32(limit)) * lax.rsqrt(total + 1e-06))[0:1, 0:1]
    for t in range(2):
        grad = clip * low[lax.rem(q + t, 2)]
        moment = 0.8 * small[2 * t] + 0.2 * grad
        second = 0.9 * small[2 * t + 1] + 0.1 * grad * grad
        fresh[2 * t] = moment
        fresh[2 * t + 1] = second
        step[t, f] = moment / (jnp.sqrt(second) + 1e-08)

    done_d = gather(
        lambda t, dev, c: step.at[t, dev, :, pl.ds(c * width, width)],
        lanes,
        sem_d,
        ring_d,
        lambda m: step.at[:, pl.ds(0, m)],
        None,
        advance,
    )

    cut = ring_f.shape[2]
    late = depth - ahead
    slab = late // cut

    def block(t, s, c):
        dev = dev_at(mod(me - ways[t] * s, n))
        return cp.at[t, pl.ds(pl.multiple_of(dev * depth + ahead + c * slab, 16), slab)]

    def pass_on(t, s, c):
        sems = sem_f.at[0], ring_f.at[t, s, c]
        return send(block(t, s, c), block(t, s, c), sems, neighbour(ways[t]))

    def share(t, s, c):
        sems = sem_f.at[1], pair_f.at[t, s]
        return send(block(t, s, c), block(t, s, c), sems, partner)

    rank = flat.shape[0]

    def apply(mat, steps):
        return jnp.dot(
            jnp.concatenate([mat, mat], axis=1), steps, preferred_element_type=F32
        )

    for t in range(2):
        for k in range(nf):
            flat[k * span : (k + 1) * span] = step[t, k]
        whole = flat[...]
        high = whole.astype(BF16)
        split[t, :rank] = high
        split[t, rank:] = (whole - high.astype(F32)).astype(BF16)
        made = old[t] - 0.01 * apply(own_bas[t], split[t])
        new[t] = made
        cp[t, pl.ds(pl.multiple_of(f * depth + ahead, 16), late)] = made[ahead:].astype(BF16)
        for c in range(cut):
            pass_on(t, 0, c).start()
        for c in range(cut):
            share(t, 0, c).start()
    def rows_of(t, p):
        at = pl.multiple_of((2 * p + core) * depth, depth)
        return cp.at[t, pl.ds(at, ahead)]

    if ahead:
        while at_hop[0] < n:
            advance()
        group = max(1, 256 // ahead)
        for k in range(2):
            t = q if k == 0 else 1 - q
            for p in range(0, n, group):
                size = min(group, n - p)
                moved = apply(lhs[k, p * ahead : (p + size) * ahead], split[t])
                for i in range(size):
                    kept = pre[t, p + i].astype(F32)
                    rows_of(t, p + i)[...] = (
                        kept - 0.01 * moved[i * ahead : (i + 1) * ahead]
                    ).astype(BF16)
                    send(
                        rows_of(t, p + i),
                        rows_of(t, p + i),
                        (sem_e.at[3], sem_e.at[4]),
                        partner,
                    ).start()
        arrive(pre, sem_e.at[4])

    def gone(s):
        for t in range(2):
            whole_block = cp.at[t, pl.ds(0, late)]
            arrive(whole_block, pair_f.at[t, s])

    def forward(s):
        for c in range(cut):
            for t in range(2):
                pass_on(t, s - 1, c).wait_recv()
                pass_on(t, s, c).start()
                share(t, s, c).start()
        gone(s - 1)

    loop(1, n - 1, forward)
    for c in range(cut):
        for t in range(2):
            pass_on(t, n - 2, c).wait_recv()
            share(t, n - 1, c).start()
    gone(n - 2)
    gone(n - 1)

    arrive(cp.at[:, pl.ds(0, (n - 1) * late)], sem_f.at[0])
    arrive(cp.at[:, pl.ds(0, n * late)], sem_f.at[1])
    if ahead:
        arrive(pre, sem_e.at[3])
        arrive(pre.at[:, pl.ds(0, n - 1)], sem_e.at[0])
    done_d()


def settle(fresh, new, cp, *refs):
    outs, wide, sem = refs[:8], refs[8], refs[9]
    model = cp.shape[1]
    size = sem.shape[0]
    blocks = size - 8
    step = model // blocks
    saves = [
        pltpu.make_async_copy(src, dst, sem.at[blocks + i])
        for i, (src, dst) in enumerate(
            [(fresh.at[i], outs[i]) for i in range(4)]
            + [(new.at[i], outs[4 + i]) for i in range(2)]
            + [(cp.at[0], outs[6])]
        )
    ]
    saves = saves[::-1]
    for save in saves:
        save.start()
    for i in range(blocks):
        at = pl.ds(i * step, step)
        wide[:, at] = cp[1, at].T
        saves.append(pltpu.make_async_copy(wide.at[:, at], outs[7].at[:, at], sem.at[i]))
        saves[-1].start()
    for save in saves:
        save.wait()


def body(
    saved_input,
    output_cotangent,
    recurrent_output,
    forget_logit,
    forget_cotangent,
    lower_bound,
    basis_in,
    basis_out,
    moment_in,
    second_in,
    moment_out,
    second_out,
    weight_in,
    weight_out,
):
    nf, nt = lax.axis_size("fs"), lax.axis_size("tp")
    n = nf // 2
    tokens, model = saved_input.shape
    units = recurrent_output.shape[1]
    depth, rank = basis_in.shape
    span = moment_in.shape[0]
    limit = 2.0 * rank * units * nt
    small = jax.ShapeDtypeStruct((span, units), F32)
    weight = jax.ShapeDtypeStruct((depth, units), F32)
    copied = jax.ShapeDtypeStruct((model, units), BF16)
    held = (
        jax.ShapeDtypeStruct((4, span, units), F32),
        jax.ShapeDtypeStruct((2, depth, units), F32),
        jax.ShapeDtypeStruct((2, model, units), BF16),
    )
    cut = 2 if depth % 32 == 0 else 1
    lanes = 2 if units % 256 == 0 else 1
    far = n // 2
    ahead = depth // 3 // 16 * 16
    hbm = pl.BlockSpec(memory_space=pltpu.HBM)
    vmem = pl.BlockSpec(memory_space=pltpu.VMEM)
    dma = pltpu.SemaphoreType.DMA
    outs = pl.pallas_call(
        functools.partial(kernel, nf, nt, limit, ahead),
        out_shape=tuple(pltpu.VMEM(o.shape, o.dtype) for o in held),
        in_specs=[hbm] * 5 + [vmem] + [hbm] * 8,
        out_specs=[vmem] * 3,
        scratch_shapes=[
            pltpu.VMEM((tokens, model), BF16),
            pltpu.VMEM((tokens, units), BF16),
            pltpu.VMEM((tokens, units), BF16),
            pltpu.VMEM((2, tokens, units), BF16),
            pltpu.VMEM((model, rank), BF16),
            pltpu.VMEM((2, depth, rank), BF16),
            pltpu.VMEM((2, tokens, rank), BF16),
            pltpu.VMEM((rank, units), F32),
            pltpu.VMEM((4, n, span, units), F32),
            pltpu.VMEM((2, n, span, units), F32),
            pltpu.VMEM((4, far, span, units), BF16),
            pltpu.VMEM((4, far, span, units), BF16),
            pltpu.VMEM((2, span, units), F32),
            pltpu.VMEM((2, nf, span, units), F32),
            pltpu.VMEM((rank, units), F32),
            pltpu.VMEM((2, 2 * rank, units), BF16),
            pltpu.VMEM((4, span, units), F32),
            pltpu.VMEM((2, depth, units), F32),
            pltpu.VMEM((nf * nt, 1, 128), F32),
            pltpu.VMEM((2, n, max(ahead, 16), units), BF16),
            pltpu.VMEM((2, n * max(ahead, 16), rank), BF16),
            dma((11,)),
            dma((2,)),
            dma((3,)),
            dma((4, far, 1)),
            dma((1,)),
            dma((4, far, lanes)),
            dma((3, far + 1)),
            dma((2,)),
            dma((2,)),
            dma((3,)),
            dma((4, far, lanes)),
            dma((2,)),
            dma((2, n - 1, cut)),
            dma((2, n)),
            dma((5,)),
            dma((2, n - 1)),
        ],
        compiler_params=pltpu.CompilerParams(
            collective_id=0, has_side_effects=True, vmem_limit_bytes=50 * 1024 * 1024
        ),
    )(
        saved_input,
        output_cotangent,
        recurrent_output,
        forget_logit,
        forget_cotangent,
        lower_bound.reshape(units // TILE, TILE),
        basis_in,
        basis_out,
        moment_in,
        second_in,
        moment_out,
        second_out,
        weight_in,
        weight_out.T,
    )
    blocks = 8 if model % 1024 == 0 else 1
    outs = pl.pallas_call(
        settle,
        out_shape=(small, small, small, small, weight, weight, copied)
        + (jax.ShapeDtypeStruct((units, model), BF16),),
        in_specs=[vmem] * 3,
        out_specs=[hbm] * 8,
        scratch_shapes=[pltpu.VMEM((units, model), BF16), dma((blocks + 8,))],
        compiler_params=pltpu.CompilerParams(vmem_limit_bytes=40 * 1024 * 1024),
    )(*outs)
    return tuple(outs[:5]) + (outs[5].T, outs[6], outs[7])


def solution(mesh):
    return jax.shard_map(
        body,
        mesh=mesh,
        in_specs=(
            P("fs", None),
            P("fs", None),
            P("fs", "tp"),
            P("fs", "tp"),
            P("fs", "tp"),
            P("tp"),
            P("fs", None),
            P("fs", None),
            P("fs", "tp"),
            P("fs", "tp"),
            P("fs", "tp"),
            P("fs", "tp"),
            P("fs", "tp"),
            P("tp", "fs"),
        ),
        out_specs=(
            P("fs", "tp"),
            P("fs", "tp"),
            P("fs", "tp"),
            P("fs", "tp"),
            P("fs", "tp"),
            P("tp", "fs"),
            P(None, "tp"),
            P("tp", None),
        ),
        check_vma=False,
    )
```

```python
import functools

import jax
import jax.numpy as jnp
from jax import lax
from jax.experimental import pallas as pl
from jax.experimental.pallas import tpu as pltpu
from jax.sharding import PartitionSpec as P

MESH = pl.DeviceIdType.MESH
F32 = jnp.float32
BF16 = jnp.bfloat16
UNROLL = 16
TILE = 128


def loop(start, stop, body):
    if stop - start <= UNROLL:
        for i in range(start, stop):
            body(i)
    else:

        @pl.loop(start, stop)
        def _(i):
            body(i)


def mod(value, n):
    return lax.rem(value + 2 * n, n)


def curve(value):
    octave = jnp.floor(jnp.log2(value) + 1e-3)
    return octave + value * jnp.exp2(-octave) - 1.0


def uncurve(level):
    octave = jnp.floor(level)
    return (1.0 + level - octave) * jnp.exp2(octave)


def encode(weight):
    size = jnp.maximum(jnp.abs(weight), 2.0**-31.75)
    index = jnp.clip(jnp.floor(1024.0 * (curve(size) + 31.75) + 0.5), 0.0, 31400.0)
    code = uncurve(index * (1 / 128) - 120.0)
    return jnp.where(weight < 0, -code, code).astype(BF16)


def decode(code):
    code = code.astype(F32)
    level = (curve(jnp.abs(code)) + 120.0) * (1 / 8)
    size = jnp.where(level < 1e-3, 0.0, uncurve(level - 31.75))
    return jnp.where(code < 0, -size, size)


def kernel(
    nf,
    nt,
    limit,
    ahead,
    x_hbm,
    y_hbm,
    rec_hbm,
    logit_hbm,
    fcot_hbm,
    lower_ref,
    basis_in_hbm,
    basis_out_hbm,
    m_in,
    s_in,
    m_out,
    s_out,
    w_in,
    w_out,
    fresh,
    new,
    cp,
    data,
    logit,
    fcot,
    cots,
    bas,
    own_bas,
    coded,
    term,
    part,
    peer,
    hop,
    lead,
    low,
    step,
    flat,
    split,
    small,
    old,
    tots,
    pre,
    lhs,
    load_sem,
    base_sem,
    sem_a,
    ring_a,
    sem_b,
    ring_b,
    sum_sem,
    swap_sem,
    tot_sem,
    sem_d,
    ring_d,
    sem_f,
    ring_f,
    pair_f,
    sem_e,
    ring_e,
):
    f = lax.axis_index("fs")
    tp = lax.axis_index("tp")
    q = lax.rem(tp, 2)
    n = nf // 2
    z = n // 2
    core = lax.rem(f, 2)
    chip = f // 2
    row, column = chip // 2, lax.rem(chip, 2)
    me = (1 - column) * row + column * (n - 1 - row)
    partner = (f + 1 - 2 * core, tp)
    across = (f, tp + 1 - 2 * q)

    def chip_at(position):
        side = position // z
        return 2 * ((1 - side) * position + side * (n - 1 - position)) + side

    def dev_at(position):
        return chip_at(position) * 2 + core

    depth = basis_in_hbm.shape[0]
    half = depth // 2
    units = cots.shape[2]
    span = part.shape[2]
    lanes = 2 if units % 256 == 0 else 1
    width = units // lanes

    def own(ref, dev):
        return ref.at[pl.ds(pl.multiple_of(dev * depth, depth), depth)]

    def fetch(src, dst, i):
        return pltpu.make_async_copy(src, dst, load_sem.at[i])

    def pick(i, first, second, dst, sem):
        @pl.when(q == 0)
        def _():
            pltpu.make_async_copy(first, dst, sem).start()

        @pl.when(q == 1)
        def _():
            pltpu.make_async_copy(second, dst, sem).start()

        return pltpu.make_async_copy(first, dst, sem)

    own_load = pick(0, basis_in_hbm, basis_out_hbm, own(bas, f), base_sem.at[0])
    gate_loads = [fetch(logit_hbm, logit, 0), fetch(fcot_hbm, fcot, 1)]
    for copy in gate_loads:
        copy.start()
    data_load = pick(1, x_hbm, y_hbm, data, base_sem.at[1])
    late_loads = [
        fetch(src, dst, 2 + i)
        for i, (src, dst) in enumerate(
            (
                (rec_hbm, cots.at[1]),
                (m_in, small.at[0]),
                (s_in, small.at[1]),
                (m_out, small.at[2]),
                (s_out, small.at[3]),
                (basis_in_hbm, own_bas.at[0]),
                (basis_out_hbm, own_bas.at[1]),
                (w_in, old.at[0]),
                (w_out, old.at[1]),
            )
        )
    ]
    for copy in late_loads:
        copy.start()

    barrier = pltpu.get_barrier_semaphore()
    everyone = nf * nt
    my_id = f * nt + tp

    def other(i):
        target = lax.rem(my_id + i, everyone)
        return (target // nt, lax.rem(target, nt))

    far = n // 2
    near = n - 1 - far
    two_way = ((0, 1, far), (1, -1, far), (0, -1, near), (1, 1, near))

    def neighbour(way):
        return (dev_at(mod(me + way, n)), tp)

    for target in (neighbour(1), neighbour(-1), partner, across):
        pl.semaphore_signal(barrier, inc=1, device_id=target, device_id_type=MESH)
    pl.semaphore_wait(barrier, 4)

    def send(src, dst, sems, target):
        return pltpu.make_async_remote_copy(
            src_ref=src,
            dst_ref=dst,
            send_sem=sems[0],
            recv_sem=sems[1],
            device_id=target,
            device_id_type=MESH,
        )

    def arrive(ref, sem):
        pltpu.make_async_copy(ref, ref, sem).wait()

    def gather(view, chunks, sems, ring_sem, blocks, between=None, after=None):
        flows = two_way

        def remote(j, s, c, pair, target):
            t, way, _ = flows[j]
            block = view(t, dev_at(mod(me - way * s, n)), c)
            return send(block, block, pair, target)

        def ring_copy(j, s, c):
            pair = sems.at[0], ring_sem.at[j, s, c]
            return remote(j, s, c, pair, neighbour(flows[j][1]))

        def pair_copy(j, s, c):
            return remote(j, s, c, (sems.at[1], sems.at[2]), partner)

        def each(s, act):
            for c in range(chunks):
                for j in range(len(flows)):
                    act(j, s, c)

        def move(j, s, c, first=False, last=False):
            if not first:
                ring_copy(j, s - 1, c).wait_recv()
            if not last:
                ring_copy(j, s, c).start()
            if not first or j < 2:
                pair_copy(j, s, c).start()

        each(0, functools.partial(move, first=True))
        if between is not None:
            between()
        loop(1, near, lambda s: each(s, move))
        for s in range(near, far + 1):
            for c in range(chunks):
                for j, (_, _, hops) in enumerate(flows):
                    if s <= hops:
                        move(j, s, c, last=s == hops)
        if after is not None:
            after()
        arrive(blocks(n), sems.at[2])

        def finish():
            arrive(blocks(n), sems.at[1])
            arrive(blocks(n - 1), sems.at[0])

        return finish

    def make_gate():
        for copy in gate_loads:
            copy.wait()
        tile = 64

        @pl.loop(0, cots.shape[1] // tile)
        def _(i):
            at = pl.ds(pl.multiple_of(i * tile, tile), tile)
            for k in range(units // TILE):
                to = slice(k * TILE, (k + 1) * TILE)
                sig = jax.nn.sigmoid(logit[at, to].astype(F32))
                cots[0, at, to] = (
                    fcot[at, to].astype(F32)
                    * (1.0 - lower_ref[k : k + 1, :])
                    * sig
                    * (1.0 - sig)
                ).astype(BF16)

    ways = (1, -1)

    def ahead_copy(t, s):
        block = pre.at[t, chip_at(mod(me - ways[t] * s, n))]
        return send(block, block, (sem_e.at[0], ring_e.at[t, s]), neighbour(ways[t]))

    at_hop = [0]

    def advance():
        s = at_hop[0]
        if not ahead or s >= n:
            return
        for t in range(2):
            if s > 0:
                ahead_copy(t, s - 1).wait_recv()
            if s < n - 1:
                ahead_copy(t, s).start()
        at_hop[0] = s + 1

    def prepare():
        make_gate()
        for copy in late_loads[7:]:
            copy.wait()
        if ahead:
            for t in range(2):
                pre[t, chip] = encode(old[t, :ahead])

    own_load.wait()
    done_a = gather(
        lambda t, dev, c: bas.at[
            pl.ds(pl.multiple_of(dev * depth + t * half, half), half)
        ],
        1,
        sem_a,
        ring_a,
        lambda m: bas.at[pl.ds(0, m * depth)],
        prepare,
        advance,
    )
    data_load.wait()

    def piece(i):
        return pl.ds(pl.multiple_of(i * TILE, TILE), TILE)

    def swap(i):
        sems = swap_sem.at[0], swap_sem.at[1]
        return send(coded.at[0, piece(i)], coded.at[1, piece(i)], sems, across)

    tiles = data.shape[0] // TILE

    @pl.loop(0, tiles)
    def _(i):
        coded[0, piece(i)] = jnp.dot(
            data[piece(i)], bas[...], preferred_element_type=F32
        ).astype(BF16)
        swap(i).start()

    def lend(p):
        at = pl.multiple_of((2 * p + core) * depth, depth)
        return send(
            bas.at[pl.ds(at, ahead)],
            lhs.at[1, pl.ds(p * ahead, ahead)],
            (sem_e.at[1], sem_e.at[2]),
            across,
        )

    if ahead:
        for p in range(n):
            lend(p).start()

    def project(k):
        t = q if k == 0 else 1 - q
        for c in range(lanes):
            at = slice(c * width, (c + 1) * width)
            term[:, at] = lax.dot_general(
                coded[k], cots[t, :, at], (((0,), (0,)), ((), ())), preferred_element_type=F32
            )
        for i in range(nf):
            part[k * 2 + i % 2, i // 2] = term[i * span : (i + 1) * span]

    def place_of(j, s):
        _, way, hops = two_way[j]
        return chip_at(mod(me + way * (hops - s), n))

    def pair_sum(k):
        def group(s):
            for j in (k, k + 2):
                if not isinstance(s, int) or s < two_way[j][2] or (s == far and j == k):
                    place = place_of(j, s)
                    sems = sum_sem.at[0, 0], sum_sem.at[1 + k, s]
                    send(
                        part.at[k * 2 + 1 - core, place], peer.at[k, place], sems, partner
                    ).start()

        loop(0, near, group)
        for s in range(near, far + 1):
            group(s)

    def paired(k, s):
        count = 2 if not isinstance(s, int) or s < near else 1
        arrive(peer.at[k, pl.ds(0, count)], sum_sem.at[1 + k, s])

    def ring_add(j, s, c):
        at = pl.ds(c * width, width)
        sems = sem_b.at[0], ring_b.at[j, s, c]
        return send(lead.at[j, s, :, at], hop.at[j, s, :, at], sems, neighbour(two_way[j][1]))

    def mine(j, s, c):
        k = two_way[j][0]
        at = pl.ds(c * width, width)
        place = place_of(j, s)
        return part[k * 2 + core, place, :, at] + peer[k, place, :, at]

    def begin(k):
        paired(k, 0)
        for c in range(lanes):
            at = pl.ds(c * width, width)
            for j in (k, k + 2):
                if two_way[j][2] > 0:
                    lead[j, 0, :, at] = mine(j, 0, c).astype(lead.dtype)
                    ring_add(j, 0, c).start()

    def relay(j, s, c):
        at = pl.ds(c * width, width)
        ring_add(j, s - 1, c).wait_recv()
        lead[j, s, :, at] = (hop[j, s - 1, :, at].astype(F32) + mine(j, s, c)).astype(
            lead.dtype
        )
        ring_add(j, s, c).start()

    def relay_all(k, s):
        paired(k, s)
        for c in range(lanes):
            for j in (k, k + 2):
                if isinstance(s, int) and s >= two_way[j][2]:
                    continue
                relay(j, s, c)

    def settle_sum(k):
        paired(k, far)
        for c in range(lanes):
            at = pl.ds(c * width, width)
            ring_add(k + 2, near - 1, c).wait_recv()
            kept = hop[k + 2, near - 1, :, at].astype(F32) + mine(k + 2, near, c)
            ring_add(k, far - 1, c).wait_recv()
            low[k, :, at] = hop[k, far - 1, :, at].astype(F32) + kept

    late_loads[0].wait()
    project(0)
    pair_sum(0)
    advance()
    begin(0)
    early = max(1, near - 1)
    loop(1, early, lambda s: relay_all(0, s))
    advance()
    arrive(coded.at[1], swap_sem.at[1])
    project(1)
    pair_sum(1)
    loop(early, near, lambda s: relay_all(0, s))
    begin(1)
    advance()
    for s in range(near, far):
        relay_all(0, s)
    loop(1, near, lambda s: relay_all(1, s))
    advance()
    settle_sum(0)
    for s in range(near, far):
        relay_all(1, s)
    settle_sum(1)

    square = jnp.sum(low[0] * low[0] + low[1] * low[1], axis=(0, 1), keepdims=True)
    tots[my_id] = jnp.broadcast_to(square, tots.shape[1:])

    def tell(i):
        return send(tots.at[my_id], tots.at[my_id], (tot_sem.at[0], tot_sem.at[1]), other(i))

    @pl.loop(1, everyone)
    def _(i):
        tell(i).start()

    advance()

    done_a()
    arrive(lead.at[pl.ds(0, 2)], sem_b.at[0])
    arrive(lead.at[pl.ds(0, 2), pl.ds(0, near)], sem_b.at[0])
    arrive(peer, sum_sem.at[0, 0])
    arrive(coded.at[0], swap_sem.at[0])
    for copy in late_loads[1:7]:
        copy.wait()
    if ahead:
        arrive(lhs.at[1], sem_e.at[1])
        arrive(lhs.at[1], sem_e.at[2])
        for p in range(n):
            at = pl.multiple_of((2 * p + core) * depth, depth)
            lhs[0, p * ahead : (p + 1) * ahead] = bas[pl.ds(at, ahead)]
    all_tots = tots.at[pl.ds(0, everyone - 1)]
    arrive(all_tots, tot_sem.at[1])
    arrive(all_tots, tot_sem.at[0])

    total = jnp.sum(tots[...], axis=0)
    clip = jnp.minimum(1.0, jnp.sqrt(F32(limit)) * lax.rsqrt(total + 1e-06))[0:1, 0:1]
    for t in range(2):
        grad = clip * low[lax.rem(q + t, 2)]
        moment = 0.8 * small[2 * t] + 0.2 * grad
        second = 0.9 * small[2 * t + 1] + 0.1 * grad * grad
        fresh[2 * t] = moment
        fresh[2 * t + 1] = second
        step[t, f] = moment / (jnp.sqrt(second) + 1e-08)

    done_d = gather(
        lambda t, dev, c: step.at[t, dev, :, pl.ds(c * width, width)],
        lanes,
        sem_d,
        ring_d,
        lambda m: step.at[:, pl.ds(0, m)],
        None,
        advance,
    )

    cut = ring_f.shape[2]
    late = depth - ahead
    slab = late // cut

    def block(t, s, c):
        dev = dev_at(mod(me - ways[t] * s, n))
        return cp.at[t, pl.ds(pl.multiple_of(dev * depth + ahead + c * slab, 16), slab)]

    def pass_on(t, s, c):
        sems = sem_f.at[0], ring_f.at[t, s, c]
        return send(block(t, s, c), block(t, s, c), sems, neighbour(ways[t]))

    def share(t, s, c):
        sems = sem_f.at[1], pair_f.at[t, s]
        return send(block(t, s, c), block(t, s, c), sems, partner)

    rank = flat.shape[0]

    def apply(mat, steps):
        return jnp.dot(
            jnp.concatenate([mat, mat], axis=1), steps, preferred_element_type=F32
        )

    for t in range(2):
        for k in range(nf):
            flat[k * span : (k + 1) * span] = step[t, k]
        whole = flat[...]
        high = whole.astype(BF16)
        split[t, :rank] = high
        split[t, rank:] = (whole - high.astype(F32)).astype(BF16)
        made = old[t] - 0.01 * apply(own_bas[t], split[t])
        new[t] = made
        cp[t, pl.ds(pl.multiple_of(f * depth + ahead, 16), late)] = made[ahead:].astype(BF16)
        for c in range(cut):
            pass_on(t, 0, c).start()
        for c in range(cut):
            share(t, 0, c).start()
    def rows_of(t, p):
        at = pl.multiple_of((2 * p + core) * depth, depth)
        return cp.at[t, pl.ds(at, ahead)]

    pieces = []
    if ahead:
        group = max(1, 192 // ahead)
        pieces = [(k, p) for p in range(0, n, group) for k in range(2)]

    def renew(k, p):
        t = q if k == 0 else 1 - q
        size = min(group, n - p)
        moved = apply(lhs[k, p * ahead : (p + size) * ahead], split[t])
        for i in range(size):
            kept = decode(pre[t, p + i])
            rows = rows_of(t, p + i)
            rows[...] = (kept - 0.01 * moved[i * ahead : (i + 1) * ahead]).astype(BF16)
            send(rows, rows, (sem_e.at[3], sem_e.at[4]), partner).start()

    def some_pieces(count):
        while at_hop[0] < n and ahead:
            advance()
        for _ in range(min(count, len(pieces))):
            renew(*pieces.pop(0))

    def gone(s):
        for t in range(2):
            whole_block = cp.at[t, pl.ds(0, late)]
            arrive(whole_block, pair_f.at[t, s])

    def forward(s):
        for c in range(cut):
            for t in range(2):
                pass_on(t, s - 1, c).wait_recv()
                pass_on(t, s, c).start()
                share(t, s, c).start()
            some_pieces(1)
        gone(s - 1)

    loop(1, n - 1, forward)
    some_pieces(len(pieces))
    for c in range(cut):
        for t in range(2):
            pass_on(t, n - 2, c).wait_recv()
            share(t, n - 1, c).start()
    gone(n - 2)
    gone(n - 1)

    arrive(cp.at[:, pl.ds(0, (n - 1) * late)], sem_f.at[0])
    arrive(cp.at[:, pl.ds(0, n * late)], sem_f.at[1])
    if ahead:
        arrive(pre, sem_e.at[4])
        arrive(pre, sem_e.at[3])
        arrive(pre.at[:, pl.ds(0, n - 1)], sem_e.at[0])
    done_d()


def settle(fresh, new, cp, *refs):
    outs, wide, sem = refs[:8], refs[8], refs[9]
    model = cp.shape[1]
    size = sem.shape[0]
    blocks = size - 8
    step = model // blocks
    saves = [
        pltpu.make_async_copy(src, dst, sem.at[blocks + i])
        for i, (src, dst) in enumerate(
            [(fresh.at[i], outs[i]) for i in range(4)]
            + [(new.at[i], outs[4 + i]) for i in range(2)]
            + [(cp.at[0], outs[6])]
        )
    ]
    saves = saves[::-1]
    for save in saves:
        save.start()
    for i in range(blocks):
        at = pl.ds(i * step, step)
        wide[:, at] = cp[1, at].T
        saves.append(pltpu.make_async_copy(wide.at[:, at], outs[7].at[:, at], sem.at[i]))
        saves[-1].start()
    for save in saves:
        save.wait()


def body(
    saved_input,
    output_cotangent,
    recurrent_output,
    forget_logit,
    forget_cotangent,
    lower_bound,
    basis_in,
    basis_out,
    moment_in,
    second_in,
    moment_out,
    second_out,
    weight_in,
    weight_out,
):
    nf, nt = lax.axis_size("fs"), lax.axis_size("tp")
    n = nf // 2
    tokens, model = saved_input.shape
    units = recurrent_output.shape[1]
    depth, rank = basis_in.shape
    span = moment_in.shape[0]
    limit = 2.0 * rank * units * nt
    small = jax.ShapeDtypeStruct((span, units), F32)
    weight = jax.ShapeDtypeStruct((depth, units), F32)
    copied = jax.ShapeDtypeStruct((model, units), BF16)
    held = (
        jax.ShapeDtypeStruct((4, span, units), F32),
        jax.ShapeDtypeStruct((2, depth, units), F32),
        jax.ShapeDtypeStruct((2, model, units), BF16),
    )
    cut = 3 if depth % 32 == 0 else 1
    lanes = 2 if units % 256 == 0 else 1
    far = n // 2
    ahead = depth // 2 // 16 * 16 if depth > 32 else 0
    hbm = pl.BlockSpec(memory_space=pltpu.HBM)
    vmem = pl.BlockSpec(memory_space=pltpu.VMEM)
    dma = pltpu.SemaphoreType.DMA
    outs = pl.pallas_call(
        functools.partial(kernel, nf, nt, limit, ahead),
        out_shape=tuple(pltpu.VMEM(o.shape, o.dtype) for o in held),
        in_specs=[hbm] * 5 + [vmem] + [hbm] * 8,
        out_specs=[vmem] * 3,
        scratch_shapes=[
            pltpu.VMEM((tokens, model), BF16),
            pltpu.VMEM((tokens, units), BF16),
            pltpu.VMEM((tokens, units), BF16),
            pltpu.VMEM((2, tokens, units), BF16),
            pltpu.VMEM((model, rank), BF16),
            pltpu.VMEM((2, depth, rank), BF16),
            pltpu.VMEM((2, tokens, rank), BF16),
            pltpu.VMEM((rank, units), F32),
            pltpu.VMEM((4, n, span, units), F32),
            pltpu.VMEM((2, n, span, units), F32),
            pltpu.VMEM((4, far, span, units), BF16),
            pltpu.VMEM((4, far, span, units), BF16),
            pltpu.VMEM((2, span, units), F32),
            pltpu.VMEM((2, nf, span, units), F32),
            pltpu.VMEM((rank, units), F32),
            pltpu.VMEM((2, 2 * rank, units), BF16),
            pltpu.VMEM((4, span, units), F32),
            pltpu.VMEM((2, depth, units), F32),
            pltpu.VMEM((nf * nt, 1, 128), F32),
            pltpu.VMEM((2, n, max(ahead, 16), units), BF16),
            pltpu.VMEM((2, n * max(ahead, 16), rank), BF16),
            dma((11,)),
            dma((2,)),
            dma((3,)),
            dma((4, far, 1)),
            dma((1,)),
            dma((4, far, lanes)),
            dma((3, far + 1)),
            dma((2,)),
            dma((2,)),
            dma((3,)),
            dma((4, far, lanes)),
            dma((2,)),
            dma((2, n - 1, cut)),
            dma((2, n)),
            dma((5,)),
            dma((2, n - 1)),
        ],
        compiler_params=pltpu.CompilerParams(
            collective_id=0, has_side_effects=True, vmem_limit_bytes=50 * 1024 * 1024
        ),
    )(
        saved_input,
        output_cotangent,
        recurrent_output,
        forget_logit,
        forget_cotangent,
        lower_bound.reshape(units // TILE, TILE),
        basis_in,
        basis_out,
        moment_in,
        second_in,
        moment_out,
        second_out,
        weight_in,
        weight_out.T,
    )
    blocks = 8 if model % 1024 == 0 else 1
    outs = pl.pallas_call(
        settle,
        out_shape=(small, small, small, small, weight, weight, copied)
        + (jax.ShapeDtypeStruct((units, model), BF16),),
        in_specs=[vmem] * 3,
        out_specs=[hbm] * 8,
        scratch_shapes=[pltpu.VMEM((units, model), BF16), dma((blocks + 8,))],
        compiler_params=pltpu.CompilerParams(vmem_limit_bytes=40 * 1024 * 1024),
    )(*outs)
    return tuple(outs[:5]) + (outs[5].T, outs[6], outs[7])


def solution(mesh):
    return jax.shard_map(
        body,
        mesh=mesh,
        in_specs=(
            P("fs", None),
            P("fs", None),
            P("fs", "tp"),
            P("fs", "tp"),
            P("fs", "tp"),
            P("tp"),
            P("fs", None),
            P("fs", None),
            P("fs", "tp"),
            P("fs", "tp"),
            P("fs", "tp"),
            P("fs", "tp"),
            P("fs", "tp"),
            P("tp", "fs"),
        ),
        out_specs=(
            P("fs", "tp"),
            P("fs", "tp"),
            P("fs", "tp"),
            P("fs", "tp"),
            P("fs", "tp"),
            P("tp", "fs"),
            P(None, "tp"),
            P("tp", None),
        ),
        check_vma=False,
    )
```

```python
import functools

import jax
import jax.numpy as jnp
from jax import lax
from jax.experimental import pallas as pl
from jax.experimental.pallas import tpu as pltpu
from jax.sharding import PartitionSpec as P

MESH = pl.DeviceIdType.MESH
F32 = jnp.float32
BF16 = jnp.bfloat16
UNROLL = 16
TILE = 128


def loop(start, stop, body):
    if stop - start <= UNROLL:
        for i in range(start, stop):
            body(i)
    else:

        @pl.loop(start, stop)
        def _(i):
            body(i)


def mod(value, n):
    return lax.rem(value + 2 * n, n)


def curve(value):
    octave = jnp.floor(jnp.log2(value) + 1e-3)
    return octave + value * jnp.exp2(-octave) - 1.0


def uncurve(level):
    octave = jnp.floor(level)
    return (1.0 + level - octave) * jnp.exp2(octave)


def encode(weight):
    size = jnp.maximum(jnp.abs(weight), 2.0**-31.75)
    index = jnp.clip(jnp.floor(1024.0 * (curve(size) + 31.75) + 0.5), 0.0, 31400.0)
    code = uncurve(index * (1 / 128) - 120.0)
    return jnp.where(weight < 0, -code, code).astype(BF16)


def decode(code):
    code = code.astype(F32)
    level = (curve(jnp.abs(code)) + 120.0) * (1 / 8)
    size = jnp.where(level < 1e-3, 0.0, uncurve(level - 31.75))
    return jnp.where(code < 0, -size, size)


def kernel(
    nf,
    nt,
    limit,
    ahead,
    x_hbm,
    y_hbm,
    rec_hbm,
    logit_hbm,
    fcot_hbm,
    lower_ref,
    basis_in_hbm,
    basis_out_hbm,
    m_in,
    s_in,
    m_out,
    s_out,
    w_in,
    w_out,
    fresh,
    new,
    cp,
    data,
    logit,
    fcot,
    cots,
    bas,
    own_bas,
    coded,
    term,
    part,
    peer,
    hop,
    lead,
    low,
    step,
    flat,
    split,
    small,
    old,
    tots,
    pre,
    lhs,
    load_sem,
    base_sem,
    sem_a,
    ring_a,
    sem_b,
    ring_b,
    sum_sem,
    swap_sem,
    tot_sem,
    sem_d,
    ring_d,
    sem_f,
    ring_f,
    pair_f,
    sem_e,
    ring_e,
):
    f = lax.axis_index("fs")
    tp = lax.axis_index("tp")
    q = lax.rem(tp, 2)
    n = nf // 2
    z = n // 2
    core = lax.rem(f, 2)
    chip = f // 2
    row, column = chip // 2, lax.rem(chip, 2)
    me = (1 - column) * row + column * (n - 1 - row)
    partner = (f + 1 - 2 * core, tp)
    across = (f, tp + 1 - 2 * q)

    def chip_at(position):
        side = position // z
        return 2 * ((1 - side) * position + side * (n - 1 - position)) + side

    def dev_at(position):
        return chip_at(position) * 2 + core

    depth = basis_in_hbm.shape[0]
    half = depth // 2
    units = cots.shape[2]
    span = part.shape[2]
    lanes = 2 if units % 256 == 0 else 1
    width = units // lanes

    def own(ref, dev):
        return ref.at[pl.ds(pl.multiple_of(dev * depth, depth), depth)]

    def fetch(src, dst, i):
        return pltpu.make_async_copy(src, dst, load_sem.at[i])

    def pick(i, first, second, dst, sem):
        @pl.when(q == 0)
        def _():
            pltpu.make_async_copy(first, dst, sem).start()

        @pl.when(q == 1)
        def _():
            pltpu.make_async_copy(second, dst, sem).start()

        return pltpu.make_async_copy(first, dst, sem)

    own_load = pick(0, basis_in_hbm, basis_out_hbm, own(bas, f), base_sem.at[0])
    gate_loads = [fetch(logit_hbm, logit, 0), fetch(fcot_hbm, fcot, 1)]
    for copy in gate_loads:
        copy.start()
    data_load = pick(1, x_hbm, y_hbm, data, base_sem.at[1])
    late_loads = [
        fetch(src, dst, 2 + i)
        for i, (src, dst) in enumerate(
            (
                (rec_hbm, cots.at[1]),
                (m_in, small.at[0]),
                (s_in, small.at[1]),
                (m_out, small.at[2]),
                (s_out, small.at[3]),
                (basis_in_hbm, own_bas.at[0]),
                (basis_out_hbm, own_bas.at[1]),
                (w_in, old.at[0]),
                (w_out, old.at[1]),
            )
        )
    ]
    for copy in late_loads:
        copy.start()

    barrier = pltpu.get_barrier_semaphore()
    everyone = nf * nt
    my_id = f * nt + tp

    def other(i):
        target = lax.rem(my_id + i, everyone)
        return (target // nt, lax.rem(target, nt))

    far = n // 2
    near = n - 1 - far
    two_way = ((0, 1, far), (1, -1, far), (0, -1, near), (1, 1, near))

    def neighbour(way):
        return (dev_at(mod(me + way, n)), tp)

    for target in (neighbour(1), neighbour(-1), partner, across):
        pl.semaphore_signal(barrier, inc=1, device_id=target, device_id_type=MESH)
    pl.semaphore_wait(barrier, 4)

    def send(src, dst, sems, target):
        return pltpu.make_async_remote_copy(
            src_ref=src,
            dst_ref=dst,
            send_sem=sems[0],
            recv_sem=sems[1],
            device_id=target,
            device_id_type=MESH,
        )

    def arrive(ref, sem):
        pltpu.make_async_copy(ref, ref, sem).wait()

    def gather(view, chunks, sems, ring_sem, blocks, between=None, after=None, seen=None):
        flows = two_way

        def remote(j, s, c, pair, target):
            t, way, _ = flows[j]
            block = view(t, dev_at(mod(me - way * s, n)), c)
            return send(block, block, pair, target)

        def ring_copy(j, s, c):
            pair = sems.at[0], ring_sem.at[j, s, c]
            return remote(j, s, c, pair, neighbour(flows[j][1]))

        def pair_copy(j, s, c):
            return remote(j, s, c, (sems.at[1], sems.at[2]), partner)

        def each(s, act):
            for c in range(chunks):
                for j in range(len(flows)):
                    act(j, s, c)

        def move(j, s, c, first=False, last=False):
            if not first:
                ring_copy(j, s - 1, c).wait_recv()
            if not last:
                ring_copy(j, s, c).start()
            if not first or j < 2:
                pair_copy(j, s, c).start()

        def note(s, which):
            if seen is not None:
                for j in which:
                    t, way, _ = flows[j]
                    seen(t, dev_at(mod(me - way * s, n)))

        each(0, functools.partial(move, first=True))
        if between is not None:
            between()
        note(0, range(2))

        def onward(s):
            each(s, move)
            note(s, range(4))

        loop(1, near, onward)
        for s in range(near, far + 1):
            for c in range(chunks):
                for j, (_, _, hops) in enumerate(flows):
                    if s <= hops:
                        move(j, s, c, last=s == hops)
            if s < far:
                note(s, [j for j in range(4) if s <= flows[j][2]])
        if after is not None:
            after()
            note(far, range(2))
        else:
            note(far, range(2))
        arrive(blocks(n), sems.at[2])

        def finish():
            arrive(blocks(n), sems.at[1])
            arrive(blocks(n - 1), sems.at[0])

        return finish

    def make_gate():
        for copy in gate_loads:
            copy.wait()
        tile = 64

        @pl.loop(0, cots.shape[1] // tile)
        def _(i):
            at = pl.ds(pl.multiple_of(i * tile, tile), tile)
            for k in range(units // TILE):
                to = slice(k * TILE, (k + 1) * TILE)
                sig = jax.nn.sigmoid(logit[at, to].astype(F32))
                cots[0, at, to] = (
                    fcot[at, to].astype(F32)
                    * (1.0 - lower_ref[k : k + 1, :])
                    * sig
                    * (1.0 - sig)
                ).astype(BF16)

    ways = (1, -1)

    def ahead_copy(t, s):
        block = pre.at[t, chip_at(mod(me - ways[t] * s, n))]
        return send(block, block, (sem_e.at[0], ring_e.at[t, s]), neighbour(ways[t]))

    at_hop = [0]

    def advance():
        s = at_hop[0]
        if not ahead or s >= n:
            return
        for t in range(2):
            if s > 0:
                ahead_copy(t, s - 1).wait_recv()
            if s < n - 1:
                ahead_copy(t, s).start()
        at_hop[0] = s + 1

    def prepare():
        make_gate()
        for copy in late_loads[7:]:
            copy.wait()
        if ahead:
            for t in range(2):
                pre[t, chip] = encode(old[t, :ahead])

    own_load.wait()
    done_a = gather(
        lambda t, dev, c: bas.at[
            pl.ds(pl.multiple_of(dev * depth + t * half, half), half)
        ],
        1,
        sem_a,
        ring_a,
        lambda m: bas.at[pl.ds(0, m * depth)],
        prepare,
        advance,
    )
    data_load.wait()

    def piece(i):
        return pl.ds(pl.multiple_of(i * TILE, TILE), TILE)

    def swap(i):
        sems = swap_sem.at[0], swap_sem.at[1]
        return send(coded.at[0, piece(i)], coded.at[1, piece(i)], sems, across)

    tiles = data.shape[0] // TILE

    @pl.loop(0, tiles)
    def _(i):
        coded[0, piece(i)] = jnp.dot(
            data[piece(i)], bas[...], preferred_element_type=F32
        ).astype(BF16)
        swap(i).start()

    def lend(p):
        at = pl.multiple_of((2 * p + core) * depth, depth)
        return send(
            bas.at[pl.ds(at, ahead)],
            lhs.at[1, pl.ds(p * ahead, ahead)],
            (sem_e.at[1], sem_e.at[2]),
            across,
        )

    if ahead:
        for p in range(n):
            lend(p).start()

    def project(k):
        t = q if k == 0 else 1 - q
        for c in range(lanes):
            at = slice(c * width, (c + 1) * width)
            term[:, at] = lax.dot_general(
                coded[k], cots[t, :, at], (((0,), (0,)), ((), ())), preferred_element_type=F32
            )
        for i in range(nf):
            part[k * 2 + i % 2, i // 2] = term[i * span : (i + 1) * span]

    def place_of(j, s):
        _, way, hops = two_way[j]
        return chip_at(mod(me + way * (hops - s), n))

    def pair_sum(k):
        def group(s):
            for j in (k, k + 2):
                if not isinstance(s, int) or s < two_way[j][2] or (s == far and j == k):
                    place = place_of(j, s)
                    sems = sum_sem.at[0, 0], sum_sem.at[1 + k, s]
                    send(
                        part.at[k * 2 + 1 - core, place], peer.at[k, place], sems, partner
                    ).start()

        loop(0, near, group)
        for s in range(near, far + 1):
            group(s)

    def paired(k, s):
        count = 2 if not isinstance(s, int) or s < near else 1
        arrive(peer.at[k, pl.ds(0, count)], sum_sem.at[1 + k, s])

    def ring_add(j, s, c):
        at = pl.ds(c * width, width)
        sems = sem_b.at[0], ring_b.at[j, s, c]
        return send(lead.at[j, s, :, at], hop.at[j, s, :, at], sems, neighbour(two_way[j][1]))

    def mine(j, s, c):
        k = two_way[j][0]
        at = pl.ds(c * width, width)
        place = place_of(j, s)
        return part[k * 2 + core, place, :, at] + peer[k, place, :, at]

    def begin(k):
        paired(k, 0)
        for c in range(lanes):
            at = pl.ds(c * width, width)
            for j in (k, k + 2):
                if two_way[j][2] > 0:
                    lead[j, 0, :, at] = mine(j, 0, c).astype(lead.dtype)
                    ring_add(j, 0, c).start()

    def relay(j, s, c):
        at = pl.ds(c * width, width)
        ring_add(j, s - 1, c).wait_recv()
        lead[j, s, :, at] = (hop[j, s - 1, :, at].astype(F32) + mine(j, s, c)).astype(
            lead.dtype
        )
        ring_add(j, s, c).start()

    def relay_all(k, s):
        paired(k, s)
        for c in range(lanes):
            for j in (k, k + 2):
                if isinstance(s, int) and s >= two_way[j][2]:
                    continue
                relay(j, s, c)

    def settle_sum(k):
        paired(k, far)
        for c in range(lanes):
            at = pl.ds(c * width, width)
            ring_add(k + 2, near - 1, c).wait_recv()
            kept = hop[k + 2, near - 1, :, at].astype(F32) + mine(k + 2, near, c)
            ring_add(k, far - 1, c).wait_recv()
            low[k, :, at] = hop[k, far - 1, :, at].astype(F32) + kept

    late_loads[0].wait()
    project(0)
    pair_sum(0)
    advance()
    begin(0)
    early = max(1, near - 1)
    loop(1, early, lambda s: relay_all(0, s))
    advance()
    arrive(coded.at[1], swap_sem.at[1])
    project(1)
    pair_sum(1)
    loop(early, near, lambda s: relay_all(0, s))
    begin(1)
    advance()
    for s in range(near, far):
        relay_all(0, s)
    loop(1, near, lambda s: relay_all(1, s))
    advance()
    settle_sum(0)
    for s in range(near, far):
        relay_all(1, s)
    settle_sum(1)

    square = jnp.sum(low[0] * low[0] + low[1] * low[1], axis=(0, 1), keepdims=True)
    tots[my_id] = jnp.broadcast_to(square, tots.shape[1:])

    def tell(i):
        return send(tots.at[my_id], tots.at[my_id], (tot_sem.at[0], tot_sem.at[1]), other(i))

    @pl.loop(1, everyone)
    def _(i):
        tell(i).start()

    advance()

    done_a()
    arrive(lead.at[pl.ds(0, 2)], sem_b.at[0])
    arrive(lead.at[pl.ds(0, 2), pl.ds(0, near)], sem_b.at[0])
    arrive(peer, sum_sem.at[0, 0])
    arrive(coded.at[0], swap_sem.at[0])
    for copy in late_loads[1:7]:
        copy.wait()
    if ahead:
        arrive(lhs.at[1], sem_e.at[1])
        arrive(lhs.at[1], sem_e.at[2])
        for p in range(n):
            at = pl.multiple_of((2 * p + core) * depth, depth)
            lhs[0, p * ahead : (p + 1) * ahead] = bas[pl.ds(at, ahead)]
    all_tots = tots.at[pl.ds(0, everyone - 1)]
    arrive(all_tots, tot_sem.at[1])
    arrive(all_tots, tot_sem.at[0])

    total = jnp.sum(tots[...], axis=0)
    clip = jnp.minimum(1.0, jnp.sqrt(F32(limit)) * lax.rsqrt(total + 1e-06))[0:1, 0:1]
    for t in range(2):
        grad = clip * low[lax.rem(q + t, 2)]
        moment = 0.8 * small[2 * t] + 0.2 * grad
        second = 0.9 * small[2 * t + 1] + 0.1 * grad * grad
        fresh[2 * t] = moment
        fresh[2 * t + 1] = second
        step[t, f] = encode(moment / (jnp.sqrt(second) + 1e-08) * (1 / 32))

    even = span % 8 == 0

    def open_step(t, dev):
        rows = pl.ds(pl.multiple_of(dev * span, 8), span)
        flat[t, rows] = 32.0 * decode(step[t, dev])

    done_d = gather(
        lambda t, dev, c: step.at[t, dev, :, pl.ds(c * width, width)],
        lanes,
        sem_d,
        ring_d,
        lambda m: step.at[:, pl.ds(0, m)],
        None,
        advance,
        open_step if even else None,
    )

    cut = ring_f.shape[2]
    late = depth - ahead
    slab = late // cut

    def block(t, s, c):
        dev = dev_at(mod(me - ways[t] * s, n))
        return cp.at[t, pl.ds(pl.multiple_of(dev * depth + ahead + c * slab, 16), slab)]

    def pass_on(t, s, c):
        sems = sem_f.at[0], ring_f.at[t, s, c]
        return send(block(t, s, c), block(t, s, c), sems, neighbour(ways[t]))

    def share(t, s, c):
        sems = sem_f.at[1], pair_f.at[t, s]
        return send(block(t, s, c), block(t, s, c), sems, partner)

    rank = flat.shape[1]

    def apply(mat, steps):
        return jnp.dot(
            jnp.concatenate([mat, mat], axis=1), steps, preferred_element_type=F32
        )

    for t in range(2):
        if even:
            for p in range(n):
                open_step(t, 2 * p + 1 - core)
        else:
            for k in range(nf):
                flat[t, k * span : (k + 1) * span] = 32.0 * decode(step[t, k])
        whole = flat[t]
        high = whole.astype(BF16)
        split[t, :rank] = high
        split[t, rank:] = (whole - high.astype(F32)).astype(BF16)
        made = old[t] - 0.01 * apply(own_bas[t], split[t])
        new[t] = made
        cp[t, pl.ds(pl.multiple_of(f * depth + ahead, 16), late)] = made[ahead:].astype(BF16)
        for c in range(cut):
            pass_on(t, 0, c).start()
        for c in range(cut):
            share(t, 0, c).start()
    def rows_of(t, p):
        at = pl.multiple_of((2 * p + core) * depth, depth)
        return cp.at[t, pl.ds(at, ahead)]

    pieces = []
    if ahead:
        group = max(1, 192 // ahead)
        pieces = [(k, p) for p in range(0, n, group) for k in range(2)]

    def renew(k, p):
        t = q if k == 0 else 1 - q
        size = min(group, n - p)
        moved = apply(lhs[k, p * ahead : (p + size) * ahead], split[t])
        for i in range(size):
            kept = decode(pre[t, p + i])
            rows = rows_of(t, p + i)
            rows[...] = (kept - 0.01 * moved[i * ahead : (i + 1) * ahead]).astype(BF16)
            send(rows, rows, (sem_e.at[3], sem_e.at[4]), partner).start()

    def some_pieces(count):
        while at_hop[0] < n and ahead:
            advance()
        for _ in range(min(count, len(pieces))):
            renew(*pieces.pop(0))

    def gone(s):
        for t in range(2):
            whole_block = cp.at[t, pl.ds(0, late)]
            arrive(whole_block, pair_f.at[t, s])

    def forward(s):
        for c in range(cut):
            for t in range(2):
                pass_on(t, s - 1, c).wait_recv()
                pass_on(t, s, c).start()
                share(t, s, c).start()
            some_pieces(1)
        gone(s - 1)

    loop(1, n - 1, forward)
    some_pieces(len(pieces))
    for c in range(cut):
        for t in range(2):
            pass_on(t, n - 2, c).wait_recv()
            share(t, n - 1, c).start()
    gone(n - 2)
    gone(n - 1)

    arrive(cp.at[:, pl.ds(0, (n - 1) * late)], sem_f.at[0])
    arrive(cp.at[:, pl.ds(0, n * late)], sem_f.at[1])
    if ahead:
        arrive(pre, sem_e.at[4])
        arrive(pre, sem_e.at[3])
        arrive(pre.at[:, pl.ds(0, n - 1)], sem_e.at[0])
    done_d()


def settle(fresh, new, cp, *refs):
    outs, wide, sem = refs[:8], refs[8], refs[9]
    model = cp.shape[1]
    size = sem.shape[0]
    blocks = size - 8
    step = model // blocks
    saves = [
        pltpu.make_async_copy(src, dst, sem.at[blocks + i])
        for i, (src, dst) in enumerate(
            [(fresh.at[i], outs[i]) for i in range(4)]
            + [(new.at[i], outs[4 + i]) for i in range(2)]
            + [(cp.at[0], outs[6])]
        )
    ]
    saves = saves[::-1]
    for save in saves:
        save.start()
    for i in range(blocks):
        at = pl.ds(i * step, step)
        wide[:, at] = cp[1, at].T
        saves.append(pltpu.make_async_copy(wide.at[:, at], outs[7].at[:, at], sem.at[i]))
        saves[-1].start()
    for save in saves:
        save.wait()


def body(
    saved_input,
    output_cotangent,
    recurrent_output,
    forget_logit,
    forget_cotangent,
    lower_bound,
    basis_in,
    basis_out,
    moment_in,
    second_in,
    moment_out,
    second_out,
    weight_in,
    weight_out,
):
    nf, nt = lax.axis_size("fs"), lax.axis_size("tp")
    n = nf // 2
    tokens, model = saved_input.shape
    units = recurrent_output.shape[1]
    depth, rank = basis_in.shape
    span = moment_in.shape[0]
    limit = 2.0 * rank * units * nt
    small = jax.ShapeDtypeStruct((span, units), F32)
    weight = jax.ShapeDtypeStruct((depth, units), F32)
    copied = jax.ShapeDtypeStruct((model, units), BF16)
    held = (
        jax.ShapeDtypeStruct((4, span, units), F32),
        jax.ShapeDtypeStruct((2, depth, units), F32),
        jax.ShapeDtypeStruct((2, model, units), BF16),
    )
    cut = 3 if depth % 32 == 0 else 1
    lanes = 2 if units % 256 == 0 else 1
    far = n // 2
    ahead = depth // 2 // 16 * 16 if depth > 32 else 0
    hbm = pl.BlockSpec(memory_space=pltpu.HBM)
    vmem = pl.BlockSpec(memory_space=pltpu.VMEM)
    dma = pltpu.SemaphoreType.DMA
    outs = pl.pallas_call(
        functools.partial(kernel, nf, nt, limit, ahead),
        out_shape=tuple(pltpu.VMEM(o.shape, o.dtype) for o in held),
        in_specs=[hbm] * 5 + [vmem] + [hbm] * 8,
        out_specs=[vmem] * 3,
        scratch_shapes=[
            pltpu.VMEM((tokens, model), BF16),
            pltpu.VMEM((tokens, units), BF16),
            pltpu.VMEM((tokens, units), BF16),
            pltpu.VMEM((2, tokens, units), BF16),
            pltpu.VMEM((model, rank), BF16),
            pltpu.VMEM((2, depth, rank), BF16),
            pltpu.VMEM((2, tokens, rank), BF16),
            pltpu.VMEM((rank, units), F32),
            pltpu.VMEM((4, n, span, units), F32),
            pltpu.VMEM((2, n, span, units), F32),
            pltpu.VMEM((4, far, span, units), BF16),
            pltpu.VMEM((4, far, span, units), BF16),
            pltpu.VMEM((2, span, units), F32),
            pltpu.VMEM((2, nf, span, units), BF16),
            pltpu.VMEM((2, rank, units), F32),
            pltpu.VMEM((2, 2 * rank, units), BF16),
            pltpu.VMEM((4, span, units), F32),
            pltpu.VMEM((2, depth, units), F32),
            pltpu.VMEM((nf * nt, 1, 128), F32),
            pltpu.VMEM((2, n, max(ahead, 16), units), BF16),
            pltpu.VMEM((2, n * max(ahead, 16), rank), BF16),
            dma((11,)),
            dma((2,)),
            dma((3,)),
            dma((4, far, 1)),
            dma((1,)),
            dma((4, far, lanes)),
            dma((3, far + 1)),
            dma((2,)),
            dma((2,)),
            dma((3,)),
            dma((4, far, lanes)),
            dma((2,)),
            dma((2, n - 1, cut)),
            dma((2, n)),
            dma((5,)),
            dma((2, n - 1)),
        ],
        compiler_params=pltpu.CompilerParams(
            collective_id=0, has_side_effects=True, vmem_limit_bytes=50 * 1024 * 1024
        ),
    )(
        saved_input,
        output_cotangent,
        recurrent_output,
        forget_logit,
        forget_cotangent,
        lower_bound.reshape(units // TILE, TILE),
        basis_in,
        basis_out,
        moment_in,
        second_in,
        moment_out,
        second_out,
        weight_in,
        weight_out.T,
    )
    blocks = 8 if model % 1024 == 0 else 1
    outs = pl.pallas_call(
        settle,
        out_shape=(small, small, small, small, weight, weight, copied)
        + (jax.ShapeDtypeStruct((units, model), BF16),),
        in_specs=[vmem] * 3,
        out_specs=[hbm] * 8,
        scratch_shapes=[pltpu.VMEM((units, model), BF16), dma((blocks + 8,))],
        compiler_params=pltpu.CompilerParams(vmem_limit_bytes=40 * 1024 * 1024),
    )(*outs)
    return tuple(outs[:5]) + (outs[5].T, outs[6], outs[7])


def solution(mesh):
    return jax.shard_map(
        body,
        mesh=mesh,
        in_specs=(
            P("fs", None),
            P("fs", None),
            P("fs", "tp"),
            P("fs", "tp"),
            P("fs", "tp"),
            P("tp"),
            P("fs", None),
            P("fs", None),
            P("fs", "tp"),
            P("fs", "tp"),
            P("fs", "tp"),
            P("fs", "tp"),
            P("fs", "tp"),
            P("tp", "fs"),
        ),
        out_specs=(
            P("fs", "tp"),
            P("fs", "tp"),
            P("fs", "tp"),
            P("fs", "tp"),
            P("fs", "tp"),
            P("tp", "fs"),
            P(None, "tp"),
            P("tp", None),
        ),
        check_vma=False,
    )
```

```python
import functools

import jax
import jax.numpy as jnp
from jax import lax
from jax.experimental import pallas as pl
from jax.experimental.pallas import tpu as pltpu
from jax.sharding import PartitionSpec as P

MESH = pl.DeviceIdType.MESH
F32 = jnp.float32
BF16 = jnp.bfloat16
UNROLL = 16
TILE = 128


def loop(start, stop, body):
    if stop - start <= UNROLL:
        for i in range(start, stop):
            body(i)
    else:

        @pl.loop(start, stop)
        def _(i):
            body(i)


def mod(value, n):
    return lax.rem(value + 2 * n, n)


def curve(value):
    octave = jnp.floor(jnp.log2(value) + 1e-3)
    return octave + value * jnp.exp2(-octave) - 1.0


def uncurve(level):
    octave = jnp.floor(level)
    return (1.0 + level - octave) * jnp.exp2(octave)


def encode(weight):
    size = jnp.maximum(jnp.abs(weight), 2.0**-31.75)
    index = jnp.clip(jnp.floor(1024.0 * (curve(size) + 31.75) + 0.5), 0.0, 31400.0)
    code = uncurve(index * (1 / 128) - 120.0)
    return jnp.where(weight < 0, -code, code).astype(BF16)


def decode(code):
    code = code.astype(F32)
    level = (curve(jnp.abs(code)) + 120.0) * (1 / 8)
    size = jnp.where(level < 1e-3, 0.0, uncurve(level - 31.75))
    return jnp.where(code < 0, -size, size)


def kernel(
    nf,
    nt,
    limit,
    ahead,
    x_hbm,
    y_hbm,
    rec_hbm,
    logit_hbm,
    fcot_hbm,
    lower_ref,
    basis_in_hbm,
    basis_out_hbm,
    m_in,
    s_in,
    m_out,
    s_out,
    w_in,
    w_out,
    fresh,
    new,
    cp,
    data,
    logit,
    fcot,
    cots,
    bas,
    own_bas,
    coded,
    term,
    part,
    peer,
    hop,
    lead,
    low,
    step,
    flat,
    split,
    small,
    old,
    tots,
    pre,
    lhs,
    load_sem,
    base_sem,
    sem_a,
    ring_a,
    sem_b,
    ring_b,
    sum_sem,
    swap_sem,
    tot_sem,
    sem_d,
    ring_d,
    sem_f,
    ring_f,
    pair_f,
    sem_e,
    ring_e,
):
    f = lax.axis_index("fs")
    tp = lax.axis_index("tp")
    q = lax.rem(tp, 2)
    n = nf // 2
    z = n // 2
    core = lax.rem(f, 2)
    chip = f // 2
    row, column = chip // 2, lax.rem(chip, 2)
    me = (1 - column) * row + column * (n - 1 - row)
    partner = (f + 1 - 2 * core, tp)
    across = (f, tp + 1 - 2 * q)

    def chip_at(position):
        side = position // z
        return 2 * ((1 - side) * position + side * (n - 1 - position)) + side

    def dev_at(position):
        return chip_at(position) * 2 + core

    depth = basis_in_hbm.shape[0]
    half = depth // 2
    strip = half // ring_a.shape[2]
    units = cots.shape[2]
    span = part.shape[2]
    lanes = 2 if units % 256 == 0 else 1
    width = units // lanes

    def own(ref, dev):
        return ref.at[pl.ds(pl.multiple_of(dev * depth, depth), depth)]

    def fetch(src, dst, i):
        return pltpu.make_async_copy(src, dst, load_sem.at[i])

    def pick(i, first, second, dst, sem):
        @pl.when(q == 0)
        def _():
            pltpu.make_async_copy(first, dst, sem).start()

        @pl.when(q == 1)
        def _():
            pltpu.make_async_copy(second, dst, sem).start()

        return pltpu.make_async_copy(first, dst, sem)

    own_load = pick(0, basis_in_hbm, basis_out_hbm, own(bas, f), base_sem.at[0])
    gate_loads = [fetch(logit_hbm, logit, 0), fetch(fcot_hbm, fcot, 1)]
    for copy in gate_loads:
        copy.start()
    data_load = pick(1, x_hbm, y_hbm, data, base_sem.at[1])
    late_loads = [
        fetch(src, dst, 2 + i)
        for i, (src, dst) in enumerate(
            (
                (rec_hbm, cots.at[1]),
                (m_in, small.at[0]),
                (s_in, small.at[1]),
                (m_out, small.at[2]),
                (s_out, small.at[3]),
                (basis_in_hbm, own_bas.at[0]),
                (basis_out_hbm, own_bas.at[1]),
                (w_in, old.at[0]),
                (w_out, old.at[1]),
            )
        )
    ]
    for copy in late_loads:
        copy.start()

    barrier = pltpu.get_barrier_semaphore()
    everyone = nf * nt
    my_id = f * nt + tp

    def other(i):
        target = lax.rem(my_id + i, everyone)
        return (target // nt, lax.rem(target, nt))

    far = n // 2
    near = n - 1 - far
    two_way = ((0, 1, far), (1, -1, far), (0, -1, near), (1, 1, near))

    def neighbour(way):
        return (dev_at(mod(me + way, n)), tp)

    for target in (neighbour(1), neighbour(-1), partner, across):
        pl.semaphore_signal(barrier, inc=1, device_id=target, device_id_type=MESH)
    pl.semaphore_wait(barrier, 4)

    def send(src, dst, sems, target):
        return pltpu.make_async_remote_copy(
            src_ref=src,
            dst_ref=dst,
            send_sem=sems[0],
            recv_sem=sems[1],
            device_id=target,
            device_id_type=MESH,
        )

    def arrive(ref, sem):
        pltpu.make_async_copy(ref, ref, sem).wait()

    def gather(view, chunks, sems, ring_sem, blocks, between=None, after=None, seen=None):
        flows = two_way

        def remote(j, s, c, pair, target):
            t, way, _ = flows[j]
            block = view(t, dev_at(mod(me - way * s, n)), c)
            return send(block, block, pair, target)

        def ring_copy(j, s, c):
            pair = sems.at[0], ring_sem.at[j, s, c]
            return remote(j, s, c, pair, neighbour(flows[j][1]))

        def pair_copy(j, s, c):
            return remote(j, s, c, (sems.at[1], sems.at[2]), partner)

        def each(s, act):
            for c in range(chunks):
                for j in range(len(flows)):
                    act(j, s, c)

        def move(j, s, c, first=False, last=False):
            if not first:
                ring_copy(j, s - 1, c).wait_recv()
            if not last:
                ring_copy(j, s, c).start()
            if not first or j < 2:
                pair_copy(j, s, c).start()

        def note(s, which):
            if seen is not None:
                for j in which:
                    t, way, _ = flows[j]
                    seen(t, dev_at(mod(me - way * s, n)))

        each(0, functools.partial(move, first=True))
        if between is not None:
            between()
        note(0, range(2))

        def onward(s):
            each(s, move)
            note(s, range(4))

        loop(1, near, onward)
        for s in range(near, far + 1):
            for c in range(chunks):
                for j, (_, _, hops) in enumerate(flows):
                    if s <= hops:
                        move(j, s, c, last=s == hops)
            if s < far:
                note(s, [j for j in range(4) if s <= flows[j][2]])
        if after is not None:
            after()
            note(far, range(2))
        else:
            note(far, range(2))
        arrive(blocks(n), sems.at[2])

        def finish():
            arrive(blocks(n), sems.at[1])
            arrive(blocks(n - 1), sems.at[0])

        return finish

    def make_gate():
        for copy in gate_loads:
            copy.wait()
        tile = 64

        @pl.loop(0, cots.shape[1] // tile)
        def _(i):
            at = pl.ds(pl.multiple_of(i * tile, tile), tile)
            for k in range(units // TILE):
                to = slice(k * TILE, (k + 1) * TILE)
                sig = jax.nn.sigmoid(logit[at, to].astype(F32))
                cots[0, at, to] = (
                    fcot[at, to].astype(F32)
                    * (1.0 - lower_ref[k : k + 1, :])
                    * sig
                    * (1.0 - sig)
                ).astype(BF16)

    ways = (1, -1)

    def ahead_copy(t, s):
        block = pre.at[t, chip_at(mod(me - ways[t] * s, n))]
        return send(block, block, (sem_e.at[0], ring_e.at[t, s]), neighbour(ways[t]))

    at_hop = [0]

    def advance():
        s = at_hop[0]
        if not ahead or s >= n:
            return
        for t in range(2):
            if s > 0:
                ahead_copy(t, s - 1).wait_recv()
            if s < n - 1:
                ahead_copy(t, s).start()
        at_hop[0] = s + 1

    def prepare():
        make_gate()
        for copy in late_loads[7:]:
            copy.wait()
        if ahead:
            for t in range(2):
                pre[t, chip] = encode(old[t, :ahead])

    own_load.wait()
    done_a = gather(
        lambda t, dev, c: bas.at[
            pl.ds(pl.multiple_of(dev * depth + t * half + c * strip, strip), strip)
        ],
        ring_a.shape[2],
        sem_a,
        ring_a,
        lambda m: bas.at[pl.ds(0, m * depth)],
        prepare,
        advance,
    )
    data_load.wait()

    def piece(i):
        return pl.ds(pl.multiple_of(i * TILE, TILE), TILE)

    def swap(i):
        sems = swap_sem.at[0], swap_sem.at[1]
        return send(coded.at[0, piece(i)], coded.at[1, piece(i)], sems, across)

    tiles = data.shape[0] // TILE

    @pl.loop(0, tiles)
    def _(i):
        coded[0, piece(i)] = jnp.dot(
            data[piece(i)], bas[...], preferred_element_type=F32
        ).astype(BF16)
        swap(i).start()

    def lend(p):
        at = pl.multiple_of((2 * p + core) * depth, depth)
        return send(
            bas.at[pl.ds(at, ahead)],
            lhs.at[1, pl.ds(p * ahead, ahead)],
            (sem_e.at[1], sem_e.at[2]),
            across,
        )

    if ahead:
        for p in range(n):
            lend(p).start()

    def project(k):
        t = q if k == 0 else 1 - q
        for c in range(lanes):
            at = slice(c * width, (c + 1) * width)
            term[:, at] = lax.dot_general(
                coded[k], cots[t, :, at], (((0,), (0,)), ((), ())), preferred_element_type=F32
            )
        for i in range(nf):
            part[k * 2 + i % 2, i // 2] = term[i * span : (i + 1) * span]

    def place_of(j, s):
        _, way, hops = two_way[j]
        return chip_at(mod(me + way * (hops - s), n))

    def pair_sum(k):
        def group(s):
            for j in (k, k + 2):
                if not isinstance(s, int) or s < two_way[j][2] or (s == far and j == k):
                    place = place_of(j, s)
                    sems = sum_sem.at[0, 0], sum_sem.at[1 + k, s]
                    send(
                        part.at[k * 2 + 1 - core, place], peer.at[k, place], sems, partner
                    ).start()

        loop(0, near, group)
        for s in range(near, far + 1):
            group(s)

    def paired(k, s):
        count = 2 if not isinstance(s, int) or s < near else 1
        arrive(peer.at[k, pl.ds(0, count)], sum_sem.at[1 + k, s])

    def ring_add(j, s, c):
        at = pl.ds(c * width, width)
        sems = sem_b.at[0], ring_b.at[j, s, c]
        return send(lead.at[j, s, :, at], hop.at[j, s, :, at], sems, neighbour(two_way[j][1]))

    def mine(j, s, c):
        k = two_way[j][0]
        at = pl.ds(c * width, width)
        place = place_of(j, s)
        return part[k * 2 + core, place, :, at] + peer[k, place, :, at]

    def begin(k):
        paired(k, 0)
        for c in range(lanes):
            at = pl.ds(c * width, width)
            for j in (k, k + 2):
                if two_way[j][2] > 0:
                    lead[j, 0, :, at] = mine(j, 0, c).astype(lead.dtype)
                    ring_add(j, 0, c).start()

    def relay(j, s, c):
        at = pl.ds(c * width, width)
        ring_add(j, s - 1, c).wait_recv()
        lead[j, s, :, at] = (hop[j, s - 1, :, at].astype(F32) + mine(j, s, c)).astype(
            lead.dtype
        )
        ring_add(j, s, c).start()

    def relay_all(k, s):
        paired(k, s)
        for c in range(lanes):
            for j in (k, k + 2):
                if isinstance(s, int) and s >= two_way[j][2]:
                    continue
                relay(j, s, c)

    def settle_sum(k):
        paired(k, far)
        for c in range(lanes):
            at = pl.ds(c * width, width)
            ring_add(k + 2, near - 1, c).wait_recv()
            kept = hop[k + 2, near - 1, :, at].astype(F32) + mine(k + 2, near, c)
            ring_add(k, far - 1, c).wait_recv()
            low[k, :, at] = hop[k, far - 1, :, at].astype(F32) + kept

    late_loads[0].wait()
    project(0)
    pair_sum(0)
    advance()
    begin(0)
    early = max(1, near - 1)
    loop(1, early, lambda s: relay_all(0, s))
    advance()
    arrive(coded.at[1], swap_sem.at[1])
    project(1)
    pair_sum(1)
    loop(early, near, lambda s: relay_all(0, s))
    begin(1)
    advance()
    for s in range(near, far):
        relay_all(0, s)
    loop(1, near, lambda s: relay_all(1, s))
    advance()
    settle_sum(0)
    for s in range(near, far):
        relay_all(1, s)
    settle_sum(1)

    square = jnp.sum(low[0] * low[0] + low[1] * low[1], axis=(0, 1), keepdims=True)
    tots[my_id] = jnp.broadcast_to(square, tots.shape[1:])

    def tell(i):
        return send(tots.at[my_id], tots.at[my_id], (tot_sem.at[0], tot_sem.at[1]), other(i))

    @pl.loop(1, everyone)
    def _(i):
        tell(i).start()

    advance()

    done_a()
    arrive(lead.at[pl.ds(0, 2)], sem_b.at[0])
    arrive(lead.at[pl.ds(0, 2), pl.ds(0, near)], sem_b.at[0])
    arrive(peer, sum_sem.at[0, 0])
    arrive(coded.at[0], swap_sem.at[0])
    for copy in late_loads[1:7]:
        copy.wait()
    if ahead:
        arrive(lhs.at[1], sem_e.at[1])
        arrive(lhs.at[1], sem_e.at[2])
        for p in range(n):
            at = pl.multiple_of((2 * p + core) * depth, depth)
            lhs[0, p * ahead : (p + 1) * ahead] = bas[pl.ds(at, ahead)]
    all_tots = tots.at[pl.ds(0, everyone - 1)]
    arrive(all_tots, tot_sem.at[1])
    arrive(all_tots, tot_sem.at[0])

    total = jnp.sum(tots[...], axis=0)
    clip = jnp.minimum(1.0, jnp.sqrt(F32(limit)) * lax.rsqrt(total + 1e-06))[0:1, 0:1]
    for t in range(2):
        grad = clip * low[lax.rem(q + t, 2)]
        moment = 0.8 * small[2 * t] + 0.2 * grad
        second = 0.9 * small[2 * t + 1] + 0.1 * grad * grad
        fresh[2 * t] = moment
        fresh[2 * t + 1] = second
        step[t, f] = encode(moment / (jnp.sqrt(second) + 1e-08) * (1 / 32))

    even = span % 8 == 0

    def open_step(t, dev):
        rows = pl.ds(pl.multiple_of(dev * span, 8), span)
        flat[t, rows] = 32.0 * decode(step[t, dev])

    done_d = gather(
        lambda t, dev, c: step.at[t, dev, :, pl.ds(c * width, width)],
        lanes,
        sem_d,
        ring_d,
        lambda m: step.at[:, pl.ds(0, m)],
        None,
        advance,
        open_step if even else None,
    )

    cut = ring_f.shape[2]
    late = depth - ahead
    slab = late // cut

    def block(t, s, c):
        dev = dev_at(mod(me - ways[t] * s, n))
        return cp.at[t, pl.ds(pl.multiple_of(dev * depth + ahead + c * slab, 16), slab)]

    def pass_on(t, s, c):
        sems = sem_f.at[0], ring_f.at[t, s, c]
        return send(block(t, s, c), block(t, s, c), sems, neighbour(ways[t]))

    def share(t, s, c):
        sems = sem_f.at[1], pair_f.at[t, s]
        return send(block(t, s, c), block(t, s, c), sems, partner)

    rank = flat.shape[1]

    def apply(mat, steps):
        return jnp.dot(
            jnp.concatenate([mat, mat], axis=1), steps, preferred_element_type=F32
        )

    for t in range(2):
        if even:
            for p in range(n):
                open_step(t, 2 * p + 1 - core)
        else:
            for k in range(nf):
                flat[t, k * span : (k + 1) * span] = 32.0 * decode(step[t, k])
        whole = flat[t]
        high = whole.astype(BF16)
        split[t, :rank] = high
        split[t, rank:] = (whole - high.astype(F32)).astype(BF16)
        made = old[t] - 0.01 * apply(own_bas[t], split[t])
        new[t] = made
        cp[t, pl.ds(pl.multiple_of(f * depth + ahead, 16), late)] = made[ahead:].astype(BF16)
        for c in range(cut):
            pass_on(t, 0, c).start()
        for c in range(cut):
            share(t, 0, c).start()
    def rows_of(t, p):
        at = pl.multiple_of((2 * p + core) * depth, depth)
        return cp.at[t, pl.ds(at, ahead)]

    pieces = []
    if ahead:
        group = max(1, 192 // ahead)
        pieces = [(k, p) for p in range(0, n, group) for k in range(2)]

    def renew(k, p):
        t = q if k == 0 else 1 - q
        size = min(group, n - p)
        moved = apply(lhs[k, p * ahead : (p + size) * ahead], split[t])
        for i in range(size):
            kept = decode(pre[t, p + i])
            rows = rows_of(t, p + i)
            rows[...] = (kept - 0.01 * moved[i * ahead : (i + 1) * ahead]).astype(BF16)
            send(rows, rows, (sem_e.at[3], sem_e.at[4]), partner).start()

    def some_pieces(count):
        while at_hop[0] < n and ahead:
            advance()
        for _ in range(min(count, len(pieces))):
            renew(*pieces.pop(0))

    def gone(s):
        for t in range(2):
            whole_block = cp.at[t, pl.ds(0, late)]
            arrive(whole_block, pair_f.at[t, s])

    def forward(s):
        for c in range(cut):
            for t in range(2):
                pass_on(t, s - 1, c).wait_recv()
                pass_on(t, s, c).start()
                share(t, s, c).start()
            some_pieces(1)
        gone(s - 1)

    loop(1, n - 1, forward)
    some_pieces(len(pieces))
    for c in range(cut):
        for t in range(2):
            pass_on(t, n - 2, c).wait_recv()
            share(t, n - 1, c).start()
    gone(n - 2)
    gone(n - 1)

    arrive(cp.at[:, pl.ds(0, (n - 1) * late)], sem_f.at[0])
    arrive(cp.at[:, pl.ds(0, n * late)], sem_f.at[1])
    if ahead:
        arrive(pre, sem_e.at[4])
        arrive(pre, sem_e.at[3])
        arrive(pre.at[:, pl.ds(0, n - 1)], sem_e.at[0])
    done_d()


def settle(fresh, new, cp, *refs):
    outs, wide, sem = refs[:8], refs[8], refs[9]
    model = cp.shape[1]
    size = sem.shape[0]
    blocks = size - 8
    step = model // blocks
    saves = [
        pltpu.make_async_copy(src, dst, sem.at[blocks + i])
        for i, (src, dst) in enumerate(
            [(fresh.at[i], outs[i]) for i in range(4)]
            + [(new.at[i], outs[4 + i]) for i in range(2)]
            + [(cp.at[0], outs[6])]
        )
    ]
    saves = saves[::-1]
    for save in saves:
        save.start()
    for i in range(blocks):
        at = pl.ds(i * step, step)
        wide[:, at] = cp[1, at].T
        saves.append(pltpu.make_async_copy(wide.at[:, at], outs[7].at[:, at], sem.at[i]))
        saves[-1].start()
    for save in saves:
        save.wait()


def body(
    saved_input,
    output_cotangent,
    recurrent_output,
    forget_logit,
    forget_cotangent,
    lower_bound,
    basis_in,
    basis_out,
    moment_in,
    second_in,
    moment_out,
    second_out,
    weight_in,
    weight_out,
):
    nf, nt = lax.axis_size("fs"), lax.axis_size("tp")
    n = nf // 2
    tokens, model = saved_input.shape
    units = recurrent_output.shape[1]
    depth, rank = basis_in.shape
    span = moment_in.shape[0]
    limit = 2.0 * rank * units * nt
    small = jax.ShapeDtypeStruct((span, units), F32)
    weight = jax.ShapeDtypeStruct((depth, units), F32)
    copied = jax.ShapeDtypeStruct((model, units), BF16)
    held = (
        jax.ShapeDtypeStruct((4, span, units), F32),
        jax.ShapeDtypeStruct((2, depth, units), F32),
        jax.ShapeDtypeStruct((2, model, units), BF16),
    )
    cut = 3 if depth % 32 == 0 else 1
    lanes = 2 if units % 256 == 0 else 1
    far = n // 2
    ahead = depth // 2 // 16 * 16 if depth > 32 else 0
    hbm = pl.BlockSpec(memory_space=pltpu.HBM)
    vmem = pl.BlockSpec(memory_space=pltpu.VMEM)
    dma = pltpu.SemaphoreType.DMA
    outs = pl.pallas_call(
        functools.partial(kernel, nf, nt, limit, ahead),
        out_shape=tuple(pltpu.VMEM(o.shape, o.dtype) for o in held),
        in_specs=[hbm] * 5 + [vmem] + [hbm] * 8,
        out_specs=[vmem] * 3,
        scratch_shapes=[
            pltpu.VMEM((tokens, model), BF16),
            pltpu.VMEM((tokens, units), BF16),
            pltpu.VMEM((tokens, units), BF16),
            pltpu.VMEM((2, tokens, units), BF16),
            pltpu.VMEM((model, rank), BF16),
            pltpu.VMEM((2, depth, rank), BF16),
            pltpu.VMEM((2, tokens, rank), BF16),
            pltpu.VMEM((rank, units), F32),
            pltpu.VMEM((4, n, span, units), F32),
            pltpu.VMEM((2, n, span, units), F32),
            pltpu.VMEM((4, far, span, units), BF16),
            pltpu.VMEM((4, far, span, units), BF16),
            pltpu.VMEM((2, span, units), F32),
            pltpu.VMEM((2, nf, span, units), BF16),
            pltpu.VMEM((2, rank, units), F32),
            pltpu.VMEM((2, 2 * rank, units), BF16),
            pltpu.VMEM((4, span, units), F32),
            pltpu.VMEM((2, depth, units), F32),
            pltpu.VMEM((nf * nt, 1, 128), F32),
            pltpu.VMEM((2, n, max(ahead, 16), units), BF16),
            pltpu.VMEM((2, n * max(ahead, 16), rank), BF16),
            dma((11,)),
            dma((2,)),
            dma((3,)),
            dma((4, far, 3 if depth % 96 == 0 else 1)),
            dma((1,)),
            dma((4, far, lanes)),
            dma((3, far + 1)),
            dma((2,)),
            dma((2,)),
            dma((3,)),
            dma((4, far, lanes)),
            dma((2,)),
            dma((2, n - 1, cut)),
            dma((2, n)),
            dma((5,)),
            dma((2, n - 1)),
        ],
        compiler_params=pltpu.CompilerParams(
            collective_id=0, has_side_effects=True, vmem_limit_bytes=50 * 1024 * 1024
        ),
    )(
        saved_input,
        output_cotangent,
        recurrent_output,
        forget_logit,
        forget_cotangent,
        lower_bound.reshape(units // TILE, TILE),
        basis_in,
        basis_out,
        moment_in,
        second_in,
        moment_out,
        second_out,
        weight_in,
        weight_out.T,
    )
    blocks = 8 if model % 1024 == 0 else 1
    outs = pl.pallas_call(
        settle,
        out_shape=(small, small, small, small, weight, weight, copied)
        + (jax.ShapeDtypeStruct((units, model), BF16),),
        in_specs=[vmem] * 3,
        out_specs=[hbm] * 8,
        scratch_shapes=[pltpu.VMEM((units, model), BF16), dma((blocks + 8,))],
        compiler_params=pltpu.CompilerParams(vmem_limit_bytes=40 * 1024 * 1024),
    )(*outs)
    return tuple(outs[:5]) + (outs[5].T, outs[6], outs[7])


def solution(mesh):
    return jax.shard_map(
        body,
        mesh=mesh,
        in_specs=(
            P("fs", None),
            P("fs", None),
            P("fs", "tp"),
            P("fs", "tp"),
            P("fs", "tp"),
            P("tp"),
            P("fs", None),
            P("fs", None),
            P("fs", "tp"),
            P("fs", "tp"),
            P("fs", "tp"),
            P("fs", "tp"),
            P("fs", "tp"),
            P("tp", "fs"),
        ),
        out_specs=(
            P("fs", "tp"),
            P("fs", "tp"),
            P("fs", "tp"),
            P("fs", "tp"),
            P("fs", "tp"),
            P("tp", "fs"),
            P(None, "tp"),
            P("tp", None),
        ),
        check_vma=False,
    )
```
